256 devices in a mesh: ep: 16 (over y, x), tp: 16 (over z, core).
Axes of the slice: x: 4, y: 4, z: 8, core: 2. Of those that a mesh axis runs over, the one named last changes fastest.
Arguments:
- tokens: bfloat16 [512, 4096], P('ep'), may hold values from -6 to 6
- state_matrix: float32 [512, 16, 128, 128], P('ep', 'tp'), may hold values from -1.5 to 1.5
- state_norm: float32 [512, 16, 128], P('ep', 'tp'), may hold values from -4 to 4
- state_max: float32 [512, 16], P('ep', 'tp'), may hold values from -5 to 5
- mixer_gain: float32 [4096], replicated, may hold values from 0.1 to 1.9
- w_query: bfloat16 [4096, 2048], P('ep', 'tp'), may hold values from -0.09375 to 0.09375
- w_key: bfloat16 [4096, 2048], P('ep', 'tp'), may hold values from -0.09375 to 0.09375
- w_value: bfloat16 [4096, 2048], P('ep', 'tp'), may hold values from -0.09375 to 0.09375
- w_outgate: bfloat16 [4096, 2048], P('ep', 'tp'), may hold values from -0.09375 to 0.09375
- w_ingate: bfloat16 [4096, 16], replicated, may hold values from -0.09375 to 0.09375
- w_forget: bfloat16 [4096, 16], replicated, may hold values from -0.09375 to 0.09375
- forget_bias: float32 [16], replicated, may hold values from -2 to 4
- w_proj: bfloat16 [2048, 4096], P('tp', 'ep'), may hold values from -0.125 to 0.125
- ffn_gain: float32 [4096], replicated, may hold values from 0.1 to 1.9
- w_branch: bfloat16 [4096], replicated, may hold values from -0.09375 to 0.09375
- routes: int32 [512, 2], P('ep'), may hold values from 0 to 15, all different within a row; in each aligned block of 32 rows (0 to 31, 32 to 63, ...) at most 6 rows name the same one
- route_weight: float32 [512, 2], P('ep'), may hold values from 0.2 to 1
- expert_gate: bfloat16 [16, 4096, 4096], P('ep', None, 'tp'), may hold values from -0.09375 to 0.09375
- expert_up: bfloat16 [16, 4096, 4096], P('ep', None, 'tp'), may hold values from -0.09375 to 0.09375
- expert_down: bfloat16 [16, 4096, 4096], P('ep', 'tp'), may hold values from -0.09375 to 0.09375
- dense_gate: bfloat16 [4096, 8192], P('ep', 'tp'), may hold values from -0.09375 to 0.09375
- dense_up: bfloat16 [4096, 8192], P('ep', 'tp'), may hold values from -0.09375 to 0.09375
- dense_down: bfloat16 [8192, 4096], P('tp', 'ep'), may hold values from -0.0625 to 0.0625
Outputs:
- layer_out: bfloat16 [512, 4096], P('ep')
- new_matrix: float32 [512, 16, 128, 128], P('ep', 'tp')
- new_norm: float32 [512, 16, 128], P('ep', 'tp')
- new_max: float32 [512, 16], P('ep', 'tp')
The draws below stay inside these ranges and needn't reach their ends.
Inputs may be any that keep to these rules, and one draw needn't show every extreme that they name: `routes`: each row names 2 different experts. Among the rows of one index of ep (32 sequences) no expert is named more than 6 times, and in some such group one expert is named exactly 6 times.
All inputs are finite; a program needn't handle non-finite values.
Results may differ from the reference program's by a relative error of at most 0.012.
Values may be sent and summed in bfloat16 or wider, within the bound.
No kernel may reach another device: no remote copies, remote signals or barrier semaphores. Data moves between devices by JAX's collectives and lax.ppermute only.
A program may use at most 64 MiB of HBM per device.

```python
import math
import jax
import jax.numpy as jnp
import numpy as np
from jax import lax

D = 4096
HEADS = 16
HDIM = 128
MW = 2048
FFD = 8192
FFE = 4096
TOPK = 2
SEQS = 32
BATCH = 512
EXPERTS = 16
CAP = 6
N_EP = 16


def shard_levels(stream_key, shape, pieces, low, high):
    def one(axis_at, parts):
        draws = jax.random.uniform(jax.random.fold_in(jax.random.fold_in(stream_key, 6), axis_at), (parts,), jnp.float32, low / len(pieces), high / len(pieces))
        return jnp.repeat(jnp.exp(draws), shape[axis_at] // parts).reshape((-1,) + (1,) * (len(shape) - axis_at - 1))

    level = one(*pieces[0])
    for cut in pieces[1:]:
        level = level * one(*cut)
    return level


def shared_out(key, own, number, rows, amount, top, limit, slope):
    ranking = jax.random.permutation(key, amount)
    crowded, usual = load_shares(amount, rows * top, limit, slope, True), load_shares(amount, rows * top, limit, slope, False)
    places = jnp.arange(amount)

    def named(lengths, turn):
        used = int((lengths > 0).sum())
        fixed = max(1, used // 4)
        shifted = fixed + (places - fixed + turn * (used - fixed)) % max(1, amount - fixed)
        return jnp.zeros((amount,), jnp.int32).at[ranking[jnp.where(places < fixed, places, shifted)]].set(jnp.asarray(lengths, jnp.int32))

    lengths = jnp.where(number % 4 == 0, named(crowded, number // 4), named(usual, number - number // 4 - 1))
    mixed = jax.random.permutation(jax.random.fold_in(own, 3), amount)
    giver, receiver = mixed[0:amount // 2 * 2:2], mixed[1:amount // 2 * 2:2]
    slack = jnp.minimum(lengths[giver] - 1, limit - lengths[receiver]) // 2
    slack = jnp.where((giver == ranking[0]) | (receiver == ranking[0]) | (lengths[receiver] == 0), 0, jnp.maximum(slack, 0))
    shifted = jax.random.randint(jax.random.fold_in(own, 4), (amount // 2,), 0, 1 << 20) % (slack + 1)
    lengths = lengths.at[giver].add(-shifted).at[receiver].add(shifted)
    members = jnp.searchsorted(jnp.cumsum(lengths), jnp.arange(rows * top), side="right").astype(jnp.int32)
    grid = members.reshape(top, rows).T
    grid = grid[jax.random.permutation(jax.random.fold_in(own, 1), rows)]
    turn = jax.random.randint(jax.random.fold_in(own, 2), (rows, 1), 0, top)
    return jnp.take_along_axis(grid, (jnp.arange(top)[None, :] + turn) % top, axis=1)


def load_shares(number_of, total, limit, lean, full):
    portions = [(1 << 20) // math.isqrt(standing ** lean) + 1 for standing in range(1, number_of + 1)]
    largest = limit if full else min(limit, max(-(-total // number_of), total * portions[0] // sum(portions)))
    least = 1 if total - largest >= number_of - 1 else 0
    given, surplus = [largest] + [least] * (number_of - 1), total - largest - least * (number_of - 1)
    while surplus > 0:
        movable = [i for i in range(1, number_of) if given[i] < largest] or [i for i in range(1, number_of) if given[i] < limit]
        pool, left = sum([portions[i] for i in movable]), surplus
        for i in movable:
            addition = min(limit - given[i], max(1, left * portions[i] // pool), surplus)
            given[i] = given[i] + addition
            surplus = surplus - addition
    return np.array(given)


def bell_draw(stream_key, extent, spread, reach, pieces=(), held_as=jnp.bfloat16):
    result = spread * jax.random.normal(stream_key, extent, jnp.float32)
    if pieces:
        result = result * shard_levels(stream_key, extent, pieces, -0.22, 0.18)
    return jnp.clip(result, -reach, reach).astype(held_as)


def setup_inputs(seed: int = 0) -> dict:
    key_of = jax.random.split(jax.random.key(seed), 24)
    tokens = bell_draw(key_of[0], (BATCH, D), 1.0, 6.0, ((0, 16),))
    state_matrix = bell_draw(key_of[1], (BATCH, HEADS, HDIM, HDIM), 0.1, 1.5, ((0, 16), (1, 16)), jnp.float32)
    state_norm = bell_draw(key_of[2], (BATCH, HEADS, HDIM), 0.3, 4.0, ((0, 16), (1, 16)), jnp.float32)
    state_max = bell_draw(key_of[3], (BATCH, HEADS), 1.0, 5.0, ((0, 16), (1, 16)), jnp.float32)
    mixer_gain = jnp.clip(1.0 + 0.18 * jax.random.normal(key_of[4], (D,), jnp.float32), 0.1, 1.9)
    w_query = bell_draw(key_of[5], (D, MW), D ** -0.5, 0.09375, ((0, 16), (1, 16)))
    w_key = bell_draw(key_of[6], (D, MW), D ** -0.5, 0.09375, ((0, 16), (1, 16)))
    w_value = bell_draw(key_of[7], (D, MW), D ** -0.5, 0.09375, ((0, 16), (1, 16)))
    w_outgate = bell_draw(key_of[8], (D, MW), D ** -0.5, 0.09375, ((0, 16), (1, 16)))
    w_ingate = bell_draw(key_of[9], (D, HEADS), D ** -0.5, 0.09375)
    w_forget = bell_draw(key_of[10], (D, HEADS), D ** -0.5, 0.09375)
    forget_bias = jnp.clip(jax.random.uniform(key_of[11], (HEADS,), jnp.float32, -2.0, 4.0), -2.0, 4.0)
    w_proj = bell_draw(key_of[12], (MW, D), MW ** -0.5, 0.125, ((0, 16), (1, 16)))
    ffn_gain = jnp.clip(1.0 + 0.18 * jax.random.normal(key_of[13], (D,), jnp.float32), 0.1, 1.9)
    w_branch = bell_draw(key_of[14], (D,), D ** -0.5, 0.09375)
    routes_keys = jax.random.split(jax.random.fold_in(key_of[15], 1), BATCH // SEQS)
    routes_turns = jax.random.permutation(jax.random.fold_in(key_of[15], 3), BATCH // SEQS)
    routes = jax.vmap(lambda own, number: shared_out(jax.random.fold_in(key_of[15], 2), own, number, SEQS, EXPERTS, TOPK, CAP, 2))(routes_keys, routes_turns).reshape((BATCH, TOPK))
    route_weight = jnp.clip(jnp.exp(math.log(1.0) - 1.609438 * jax.random.uniform(key_of[16], (BATCH, TOPK), jnp.float32) ** shard_levels(key_of[16], (BATCH, TOPK), ((0, 16),), -0.2, 0.2)), 0.2, 1.0)
    expert_gate = bell_draw(key_of[17], (EXPERTS, D, FFE), D ** -0.5, 0.09375, ((0, 16), (2, 16)))
    expert_up = bell_draw(key_of[18], (EXPERTS, D, FFE), D ** -0.5, 0.09375, ((0, 16), (2, 16)))
    expert_down = bell_draw(key_of[19], (EXPERTS, FFE, D), FFE ** -0.5, 0.09375, ((0, 16), (1, 16)))
    dense_gate = bell_draw(key_of[20], (D, FFD), D ** -0.5, 0.09375, ((0, 16), (1, 16)))
    dense_up = bell_draw(key_of[21], (D, FFD), D ** -0.5, 0.09375, ((0, 16), (1, 16)))
    dense_down = bell_draw(key_of[22], (FFD, D), FFD ** -0.5, 0.0625, ((0, 16), (1, 16)))
    return dict(tokens=tokens, state_matrix=state_matrix, state_norm=state_norm, state_max=state_max, mixer_gain=mixer_gain, w_query=w_query, w_key=w_key, w_value=w_value, w_outgate=w_outgate, w_ingate=w_ingate, w_forget=w_forget, forget_bias=forget_bias, w_proj=w_proj, ffn_gain=ffn_gain, w_branch=w_branch, routes=routes, route_weight=route_weight, expert_gate=expert_gate, expert_up=expert_up, expert_down=expert_down, dense_gate=dense_gate, dense_up=dense_up, dense_down=dense_down)


EPS = 1e-06

def rms_scale(values, gain):
    wide = values.astype(jnp.float32)
    return wide * lax.rsqrt(lax.optimization_barrier(jnp.mean(wide * wide, axis=-1, keepdims=True)) + EPS) * gain.astype(jnp.float32)

def slot_numbers(flat_routes, experts_all):
    onehot = (flat_routes[:, None] == jnp.arange(experts_all, dtype=jnp.int32)[None, :]).astype(jnp.int32)
    before = jnp.cumsum(onehot, axis=0) - onehot
    return lax.optimization_barrier(jnp.sum(before * onehot, axis=1)).astype(jnp.int32)

def memory_step(query_all, key_all, value_all, outgate, gate_in, gate_forget, state_matrix, state_norm, state_max):
    row_count, head_count = gate_in.shape
    head_size = state_matrix.shape[-1]
    heads_q = query_all.reshape(row_count, head_count, head_size)
    heads_k = key_all.reshape(row_count, head_count, head_size) * head_size ** (-0.5)
    heads_v = value_all.reshape(row_count, head_count, head_size)
    log_keep = jax.nn.log_sigmoid(gate_forget)
    new_max = jnp.maximum(log_keep + state_max, gate_in)
    keep_factor = jnp.exp(log_keep + state_max - new_max)
    write_factor = jnp.exp(gate_in - new_max)
    new_matrix = keep_factor[:, :, None, None] * state_matrix + write_factor[:, :, None, None] * heads_k[:, :, :, None] * heads_v[:, :, None, :]
    new_norm = keep_factor[:, :, None] * state_norm + write_factor[:, :, None] * heads_k
    numer = jnp.einsum('bhk,bhkv->bhv', heads_q, new_matrix, precision=lax.Precision.HIGHEST)
    denom = lax.optimization_barrier(jnp.sum(heads_q * new_norm, axis=-1))
    cell = numer / jnp.maximum(jnp.abs(denom), 1.0)[:, :, None]
    gated = jax.nn.sigmoid(outgate.reshape(row_count, head_count, head_size)) * cell
    mixed_heads = gated.reshape(row_count, head_count * head_size).astype(jnp.bfloat16)
    return (mixed_heads, new_matrix, new_norm, new_max)

def reference(tokens, state_matrix, state_norm, state_max, mixer_gain, w_query, w_key, w_value, w_outgate, w_ingate, w_forget, forget_bias, w_proj, ffn_gain, w_branch, routes, route_weight, expert_gate, expert_up, expert_down, dense_gate, dense_up, dense_down):
    normed = rms_scale(tokens, mixer_gain).astype(jnp.bfloat16)
    query_all = jnp.dot(normed, w_query, preferred_element_type=jnp.float32)
    key_all = jnp.dot(normed, w_key, preferred_element_type=jnp.float32)
    value_all = jnp.dot(normed, w_value, preferred_element_type=jnp.float32)
    outgate = jnp.dot(normed, w_outgate, preferred_element_type=jnp.float32)
    gate_in = jnp.dot(normed, w_ingate, preferred_element_type=jnp.float32)
    gate_forget = jnp.dot(normed, w_forget, preferred_element_type=jnp.float32) + forget_bias
    mixed_heads, new_matrix, new_norm, new_max = memory_step(query_all, key_all, value_all, outgate, gate_in, gate_forget, state_matrix, state_norm, state_max)
    mixer_out = jnp.dot(mixed_heads, w_proj, preferred_element_type=jnp.float32)
    residual = (tokens.astype(jnp.float32) + mixer_out).astype(jnp.bfloat16)
    ffn_in = rms_scale(residual, ffn_gain).astype(jnp.bfloat16)
    branch_share = jax.nn.sigmoid(jnp.dot(ffn_in, w_branch, preferred_element_type=jnp.float32))
    dense_hidden = (jax.nn.silu(jnp.dot(ffn_in, dense_gate, preferred_element_type=jnp.float32)) * jnp.dot(ffn_in, dense_up, preferred_element_type=jnp.float32)).astype(jnp.bfloat16)
    dense_out = jnp.dot(dense_hidden, dense_down, preferred_element_type=jnp.float32)
    group_routes = routes.reshape(N_EP, SEQS * TOPK)
    slots = jax.vmap(lambda group_row: slot_numbers(group_row, EXPERTS))(group_routes)
    group_ids = jnp.broadcast_to(jnp.arange(N_EP, dtype=jnp.int32)[:, None], group_routes.shape)
    repeated = jnp.repeat(ffn_in, TOPK, axis=0).reshape(N_EP, SEQS * TOPK, D)
    buffers = jnp.zeros((EXPERTS, N_EP, CAP, D), jnp.bfloat16).at[group_routes, group_ids, slots].set(repeated)

    def one_expert(index):
        rows_in = buffers[index].reshape(N_EP * CAP, D)
        hidden = (jax.nn.silu(jnp.dot(rows_in, expert_gate[index], preferred_element_type=jnp.float32)) * jnp.dot(rows_in, expert_up[index], preferred_element_type=jnp.float32)).astype(jnp.bfloat16)
        return jnp.dot(hidden, expert_down[index], preferred_element_type=jnp.float32).reshape(N_EP, CAP, D)
    results = lax.map(one_expert, jnp.arange(EXPERTS, dtype=jnp.int32))
    picked = results[group_routes, group_ids, slots].reshape(N_EP * SEQS, TOPK, D)
    shares = route_weight / lax.optimization_barrier(jnp.sum(route_weight, axis=1, keepdims=True))
    expert_rows = lax.optimization_barrier(jnp.sum(shares[:, :, None] * picked, axis=1))
    total_ffn = expert_rows + branch_share[:, None] * dense_out
    layer_out = (residual.astype(jnp.float32) + total_ffn).astype(jnp.bfloat16)
    return (layer_out, new_matrix, new_norm, new_max)
```

```python
import jax
import jax.numpy as jnp
from jax import lax
from jax.sharding import PartitionSpec as P

EPS = 1e-06
BF = jnp.bfloat16
F32 = jnp.float32


def swap(parts, axis):
    return lax.all_to_all(parts, axis, 0, 0, tiled=True)


def copies(shard, axis):
    return swap(jnp.broadcast_to(shard[None], (lax.axis_size(axis), *shard.shape)), axis)


def split_exact(x):
    high = lax.reduce_precision(x, 8, 7)
    return high.astype(BF), (x - high).astype(BF)


def slot_numbers(flat_routes, experts_all):
    onehot = (flat_routes[:, None] == jnp.arange(experts_all, dtype=jnp.int32)[None, :]).astype(
        jnp.int32
    )
    before = jnp.cumsum(onehot, axis=0) - onehot
    return jnp.sum(before * onehot, axis=1)


def on_device(
    tokens,
    state_matrix,
    state_norm,
    state_max,
    mixer_gain,
    w_query,
    w_key,
    w_value,
    w_outgate,
    w_ingate,
    w_forget,
    forget_bias,
    w_proj,
    ffn_gain,
    w_branch,
    routes,
    route_weight,
    expert_gate,
    expert_up,
    expert_down,
    dense_gate,
    dense_up,
    dense_down,
):
    rows, width = tokens.shape
    n_ep, n_tp = lax.axis_size("ep"), lax.axis_size("tp")
    my_e, my_t = lax.axis_index("ep"), lax.axis_index("tp")
    cols = width // n_ep
    everyone = rows * n_ep
    cap = 6
    dot = lambda a, b: jnp.dot(a, b, preferred_element_type=F32)

    token_cols = swap(jnp.moveaxis(tokens.reshape(rows, n_ep, cols), 1, 0), "ep")

    wide = tokens.astype(F32)
    scale = lax.rsqrt(jnp.mean(wide * wide, axis=-1, keepdims=True) + EPS)
    normed = (wide * scale * mixer_gain).astype(BF)
    gate_in = lax.dynamic_slice_in_dim(dot(normed, w_ingate), my_t, 1, 1)
    gate_forget = lax.dynamic_slice_in_dim(dot(normed, w_forget) + forget_bias, my_t, 1, 1)

    flat_routes = routes.reshape(-1)
    slots = slot_numbers(flat_routes, n_ep)
    code = (flat_routes * 8 + slots).reshape(rows, 2)

    gain_cols = lax.dynamic_slice_in_dim(mixer_gain, my_e * cols, cols, 0)
    scaled = (token_cols.reshape(everyone, cols).astype(F32) * gain_cols).astype(BF)
    partial = jnp.concatenate(
        [dot(scaled, w).astype(BF) for w in (w_query, w_key, w_value, w_outgate)], axis=1
    )
    projected = swap(partial.reshape(n_ep, rows, -1), "ep").astype(F32).sum(0) * scale
    head = projected.shape[1] // 4
    query, key, value, outgate = (projected[:, i * head : (i + 1) * head] for i in range(4))

    key = key * head ** (-0.5)
    log_keep = jax.nn.log_sigmoid(gate_forget)
    new_max = jnp.maximum(log_keep + state_max, gate_in)
    keep = jnp.exp(log_keep + state_max - new_max)
    write = jnp.exp(gate_in - new_max)
    new_matrix = (
        keep[:, :, None] * state_matrix[:, 0]
        + write[:, :, None] * key[:, :, None] * value[:, None, :]
    )
    new_norm = keep * state_norm[:, 0] + write * key
    numer = jnp.einsum("bk,bkv->bv", query, new_matrix, precision=lax.Precision.HIGHEST)
    denom = jnp.sum(query * new_norm, axis=-1, keepdims=True)
    cell = numer / jnp.maximum(jnp.abs(denom), 1.0)
    mixed = (jax.nn.sigmoid(outgate) * cell).astype(BF)

    extra = jnp.pad(code.reshape(1, -1).astype(BF), ((0, 7), (0, head - 2 * rows)))
    mixed_all = copies(jnp.concatenate([mixed, extra], axis=0), "ep")
    codes_all = mixed_all[:, rows, : 2 * rows].reshape(everyone, 2).astype(jnp.int32)
    mixed_all = mixed_all[:, :rows].reshape(everyone, head)

    spread = dot(mixed_all, w_proj).astype(BF).reshape(n_tp, rows, cols)
    mixer_out = swap(spread, "tp").astype(F32).sum(0)
    token_block = lax.dynamic_index_in_dim(token_cols, my_t, 0, keepdims=False)
    resid_block = (token_block.astype(F32) + mixer_out).astype(BF)
    resid_turned = lax.ppermute(
        resid_block, ("ep", "tp"), [(a * n_tp + b, b * n_tp + a) for a in range(n_ep) for b in range(n_tp)]
    )
    resid = copies(resid_block, "tp").reshape(everyone, cols)

    resid_wide = resid.astype(F32)
    ffn_gain_cols = lax.dynamic_slice_in_dim(ffn_gain, my_e * cols, cols, 0)
    branch_cols = lax.dynamic_slice_in_dim(w_branch, my_e * cols, cols, 0)
    gained_wide = resid_wide * ffn_gain_cols
    gained = gained_wide.astype(BF)
    squares = split_exact(jnp.sum(resid_wide * resid_wide, axis=1, keepdims=True))
    branch = split_exact(jnp.sum(gained_wide * branch_cols.astype(F32), axis=1, keepdims=True))
    side = jnp.pad(jnp.concatenate([*squares, *branch], axis=1), ((0, 0), (0, 124)))
    gate_up = jnp.concatenate(
        [dot(gained, dense_gate).astype(BF), dot(gained, dense_up).astype(BF), side], axis=1
    )
    at = jnp.arange(n_ep * cap, dtype=jnp.int32)
    wanted = jnp.arange(n_ep, dtype=jnp.int32)[:, None] * 8 + (at % cap)[None, :]
    member = (
        jnp.any(codes_all[None, None, :, :] == wanted[:, :, None, None], axis=-1)
        & ((jnp.arange(everyone, dtype=jnp.int32) // rows)[None, None, :] == (at // cap)[None, :, None])
    )
    outbound = dot(member.astype(BF).reshape(n_ep * n_ep * cap, everyone), resid).astype(BF)
    arrived = swap(outbound.reshape(n_ep, n_ep * cap, cols), "ep")
    summed = swap(gate_up.reshape(n_ep, rows, -1), "ep").astype(F32).sum(0)

    units = dense_gate.shape[1]
    ffn_scale = lax.rsqrt((summed[:, 2 * units] + summed[:, 2 * units + 1])[:, None] / width + EPS)
    branch_share = jax.nn.sigmoid((summed[:, 2 * units + 2] + summed[:, 2 * units + 3])[:, None] * ffn_scale)
    hidden = (jax.nn.silu(summed[:, :units] * ffn_scale) * (summed[:, units : 2 * units] * ffn_scale)).astype(BF)
    hidden_all = copies(hidden, "ep").reshape(everyone, units)

    rows_in = jnp.moveaxis(arrived, 0, 1).reshape(n_ep * cap, width).astype(F32)
    row_scale = lax.rsqrt(jnp.mean(rows_in * rows_in, axis=-1, keepdims=True) + EPS)
    rows_in = (rows_in * row_scale * ffn_gain).astype(BF)
    expert_hidden = (jax.nn.silu(dot(rows_in, expert_gate[0])) * dot(rows_in, expert_up[0])).astype(BF)
    expert_rows = dot(expert_hidden, expert_down[0]).astype(BF).reshape(n_ep, cap, width)
    returned = swap(expert_rows, "ep").reshape(n_ep * cap, width)

    dense_back = swap(dot(hidden_all, dense_down).astype(BF).reshape(n_ep, rows, cols), "ep")
    dense_back = jnp.moveaxis(dense_back, 0, 1).reshape(rows, width).astype(F32)

    shares = route_weight / jnp.sum(route_weight, axis=1, keepdims=True)
    place = (jnp.arange(n_ep, dtype=jnp.int32)[:, None] * 8 + jnp.arange(cap, dtype=jnp.int32)[None]).reshape(-1)
    mixing = jnp.sum(jnp.where(code[:, :, None] == place[None, None, :], shares[:, :, None], 0.0), axis=1)
    expert_sum = jnp.dot(mixing, returned.astype(F32), precision=lax.Precision.HIGHEST)
    total = (expert_sum + branch_share * dense_back).astype(BF)
    total = swap(jnp.moveaxis(total.reshape(rows, n_tp, width // n_tp), 1, 0), "tp").astype(F32).sum(0)
    out_block = (resid_turned.astype(F32) + total).astype(BF)
    layer_out = jnp.moveaxis(copies(out_block, "tp"), 0, 1).reshape(rows, width)
    return (layer_out, new_matrix[:, None], new_norm[:, None], new_max)


def solution(mesh):
    in_specs = (
        P("ep", None),
        P("ep", "tp", None, None),
        P("ep", "tp", None),
        P("ep", "tp"),
        P(),
        P("ep", "tp"),
        P("ep", "tp"),
        P("ep", "tp"),
        P("ep", "tp"),
        P(),
        P(),
        P(),
        P("tp", "ep"),
        P(),
        P(),
        P("ep", None),
        P("ep", None),
        P("ep", None, "tp"),
        P("ep", None, "tp"),
        P("ep", "tp", None),
        P("ep", "tp"),
        P("ep", "tp"),
        P("tp", "ep"),
    )
    out_specs = (P("ep", None), P("ep", "tp", None, None), P("ep", "tp", None), P("ep", "tp"))
    return jax.shard_map(
        on_device, mesh=mesh, in_specs=in_specs, out_specs=out_specs, check_vma=False
    )
```

```python
import jax
import jax.numpy as jnp
from jax import lax
from jax.experimental import pallas as pl
from jax.experimental.pallas import tpu as pltpu
from jax.sharding import PartitionSpec as P

EPS = 1e-06
BF = jnp.bfloat16
F32 = jnp.float32
I32 = jnp.int32
EP, TP = 16, 16
ROWS, WIDTH, COLS, HEAD, UNITS, CAP = 32, 4096, 256, 128, 512, 6
ALL = ROWS * EP
ROUTED = 2 * CAP * EP
SIDE = ROUTED + 8 * ROWS
PACKED = SIDE + 16
CHUNKS = WIDTH // 128
BACK = CAP * CHUNKS
RETURN = BACK + 2 * ROWS
def in_hbm(x):
    return pltpu.with_memory_space_constraint(x, pltpu.HBM)


def grant(mib):
    return pltpu.CompilerParams(vmem_limit_bytes=mib * 1024 * 1024)


VMEM = pl.BlockSpec(memory_space=pltpu.VMEM)
SMEM = pl.BlockSpec(memory_space=pltpu.SMEM)
HBM = pl.BlockSpec(memory_space=pltpu.HBM)


def swap(parts, axis):
    return lax.all_to_all(parts, axis, 0, 0, tiled=True)


def copies(shard, axis):
    return swap(jnp.broadcast_to(shard[None], (lax.axis_size(axis), *shard.shape)), axis)


def mm(a, b):
    return jnp.dot(a, b, preferred_element_type=F32)


def mm_nt(a, b):
    return lax.dot_general(a, b, (((1,), (1,)), ((), ())), preferred_element_type=F32)


def cut_kernel(x_ref, o_ref, done):
    moves = [
        pltpu.make_async_copy(x_ref.at[:, pl.ds(e * COLS, COLS)], o_ref.at[e], done.at[e]) for e in range(EP)
    ]
    for move in moves:
        move.start()
    for move in moves:
        move.wait()


def cut(tokens):
    return pl.pallas_call(
        cut_kernel,
        out_shape=jax.ShapeDtypeStruct((EP, ROWS, COLS), BF),
        in_specs=[HBM],
        out_specs=VMEM,
        scratch_shapes=[pltpu.SemaphoreType.DMA((EP,))],
        compiler_params=grant(1),
    )(in_hbm(tokens))


def prepare_kernel(
    me_ref, *refs,
):
    sources, outs, scratch = refs[:10], refs[10:17], refs[17:27]
    done = refs[27]
    moves = [pltpu.make_async_copy(a, b, done.at[i]) for i, (a, b) in enumerate(zip(sources, scratch))]
    for move in moves:
        move.start()
    x_ref, gain_ref, in_ref, forget_ref, bias_ref, max_ref, norm_ref, route_ref, weight_ref, state_ref = scratch
    scale_ref, write_ref, new_max_ref, extra_ref, table_ref, old_norm_ref, old_ref = outs
    for move in moves[:-1]:
        move.wait()
    wide = x_ref[...].astype(F32)
    scale = lax.rsqrt(jnp.sum(wide * wide, axis=1, keepdims=True) / WIDTH + EPS)
    scale_ref[...] = jnp.broadcast_to(scale, (ROWS, HEAD))
    normed = (wide * scale * gain_ref[...]).astype(BF)
    head = lax.broadcasted_iota(I32, (ROWS, TP), 1) == me_ref[1]
    pick = lambda x: jnp.sum(jnp.where(head, x, 0.0), axis=1, keepdims=True)
    row = lax.broadcasted_iota(I32, (ROWS, ROWS), 0)
    lane = lax.broadcasted_iota(I32, (ROWS, ROWS), 1)
    upright = lambda x: jnp.sum(jnp.where(lane == row, x, jnp.zeros_like(x)), axis=1, keepdims=True)
    flat = lambda x: jnp.sum(jnp.where(lane == row, x, jnp.zeros_like(x)), axis=0, keepdims=True)
    gate_in = pick(mm_nt(normed, in_ref[...]))
    gate_forget = pick(mm_nt(normed, forget_ref[...]) + bias_ref[...])
    old_max = upright(max_ref[...])
    log_keep = jnp.minimum(gate_forget, 0.0) - jnp.log1p(jnp.exp(-jnp.abs(gate_forget)))
    new_max = jnp.maximum(log_keep + old_max, gate_in)
    new_max_ref[...] = flat(new_max)
    keep = jnp.broadcast_to(jnp.exp(log_keep + old_max - new_max), (ROWS, HEAD))
    write_ref[...] = jnp.broadcast_to(jnp.exp(gate_in - new_max), (ROWS, HEAD))
    old_norm_ref[...] = keep * norm_ref[...].reshape(ROWS, HEAD)

    place = lax.broadcasted_iota(I32, (ROWS, 128), 1) == (me_ref[0] % 4) * ROWS + lax.broadcasted_iota(
        I32, (ROWS, 128), 0
    )
    across = [route_ref[k : k + 1, :] for k in range(2)]
    column = [upright(x) for x in across]
    lines = []
    for k in range(2):
        same = (across[0] == column[k]).astype(I32) + (across[1] == column[k]).astype(I32)
        slot = jnp.sum(jnp.where(lane < row, same, 0), axis=1, keepdims=True)
        code = column[k] * 8 + slot
        table_ref[k : k + 1, :] = flat(code).astype(F32)
        lines.append(jnp.sum(jnp.where(place, code, 0), axis=0, keepdims=True))
    lines.append(jnp.zeros((6, 128), I32))
    extra_ref[...] = jnp.concatenate(lines, axis=0).astype(F32).astype(BF)
    weight = weight_ref[...]
    table_ref[2:4, :] = weight / jnp.sum(weight, axis=0, keepdims=True)
    moves[-1].wait()
    for r in range(ROWS):
        old_ref[r] = keep[r : r + 1] * state_ref[r, 0]


def prepare(me, *sources):
    wide = jax.ShapeDtypeStruct((ROWS, HEAD), F32)
    return pl.pallas_call(
        prepare_kernel,
        out_shape=(
            wide, wide, jax.ShapeDtypeStruct((1, ROWS), F32), jax.ShapeDtypeStruct((8, HEAD), BF),
            jax.ShapeDtypeStruct((4, ROWS), F32), wide, jax.ShapeDtypeStruct((ROWS, HEAD, HEAD), F32),
        ),
        in_specs=[SMEM] + [HBM] * 10,
        out_specs=(VMEM,) * 7,
        scratch_shapes=[pltpu.VMEM(x.shape, x.dtype) for x in sources] + [pltpu.SemaphoreType.DMA((10,))],
        compiler_params=grant(12),
    )(me, *[in_hbm(x) for x in sources])


def my_columns(ref, me_ref):
    return ref[:, pl.ds(pl.multiple_of(me_ref[0] * COLS, COLS), COLS)]


def heads_kernel(me_ref, x_ref, gain_ref, q_ref, k_ref, v_ref, g_ref, o_ref, mine_ref):
    x = (x_ref[...].reshape(ALL, COLS).astype(F32) * my_columns(gain_ref, me_ref)).astype(BF)
    for i, w in enumerate((q_ref, k_ref, v_ref, g_ref)):
        o_ref[:, :, i * HEAD : (i + 1) * HEAD] = mm(x, w[...]).astype(BF).reshape(EP, ROWS, HEAD)
    mine_ref[...] = x_ref[me_ref[1]]


def heads(me, token_cols, gain, ws):
    return pl.pallas_call(
        heads_kernel,
        out_shape=(
            jax.ShapeDtypeStruct((EP, ROWS, 4 * HEAD), BF),
            jax.ShapeDtypeStruct((ROWS, COLS), BF),
        ),
        in_specs=[SMEM] + [VMEM] * 6,
        out_specs=(VMEM, VMEM),
        compiler_params=grant(6),
    )(me, token_cols, gain, *ws)


STEP = 8


def cell_kernel(
    p_ref, scale_ref, write_ref, extra_ref, norm_ref, old_ref,
    mixed_ref, new_norm_ref, new_ref, proj, numer, gated,
):
    step = pl.program_id(0)

    @pl.when(step == 0)
    def _():
        for i in range(4):
            lanes = slice(i * HEAD, (i + 1) * HEAD)
            total = p_ref[0, :, lanes].astype(F32)
            for e in range(1, EP):
                total = total + p_ref[e, :, lanes].astype(F32)
            proj[i] = total * scale_ref[...]

    here = pl.ds(pl.multiple_of(step * STEP, STEP), STEP)
    query, key, value, outgate = (proj[i, here, :] for i in range(4))
    write = write_ref[here, :]
    key = key * HEAD ** (-0.5)
    wkey = write * key
    new_norm = norm_ref[here, :] + wkey
    new_norm_ref[here, :] = new_norm
    query_t, wkey_t = query.T, wkey.T
    for j in range(STEP):
        row = slice(j, j + 1)
        new = old_ref[step * STEP + j] + wkey_t[:, row] * value[row]
        new_ref[j, 0] = new
        numer[row, :] = jnp.sum(query_t[:, row] * new, axis=0, keepdims=True)
    denom = jnp.sum(query * new_norm, axis=1, keepdims=True)
    out = numer[...] / jnp.maximum(jnp.abs(denom), 1.0)
    gated[here, :] = jax.nn.sigmoid(outgate) * out

    @pl.when(step == ROWS // STEP - 1)
    def _():
        mixed = gated[...].astype(BF)
        extra = extra_ref[...]
        for e in range(EP):
            mixed_ref[e, :ROWS] = mixed
            mixed_ref[e, ROWS:] = extra


def cell(parts, scale, write, extra, norm, old):
    whole = lambda *shape: pl.BlockSpec(shape, lambda i: (0,) * len(shape))
    return pl.pallas_call(
        cell_kernel,
        grid=(ROWS // STEP,),
        out_shape=(
            jax.ShapeDtypeStruct((EP, ROWS + 8, HEAD), BF),
            jax.ShapeDtypeStruct((ROWS, HEAD), F32),
            jax.ShapeDtypeStruct((ROWS, 1, HEAD, HEAD), F32),
        ),
        in_specs=[VMEM] * 6,
        out_specs=(
            whole(EP, ROWS + 8, HEAD), whole(ROWS, HEAD),
            pl.BlockSpec((STEP, 1, HEAD, HEAD), lambda i: (i, 0, 0, 0)),
        ),
        scratch_shapes=[
            pltpu.VMEM((4, ROWS, HEAD), F32),
            pltpu.VMEM((STEP, HEAD), F32),
            pltpu.VMEM((ROWS, HEAD), F32),
        ],
        compiler_params=grant(6),
    )(parts, scale, write, extra, norm, old)


def settle_kernel(p_ref, base_ref, o_ref):
    total = p_ref[0].astype(F32)
    for t in range(1, TP):
        total = total + p_ref[t].astype(F32)
    out = (base_ref[...].astype(F32) + total).astype(BF)
    for t in range(TP):
        o_ref[t] = out


def settle(parts, base):
    return pl.pallas_call(
        settle_kernel,
        out_shape=jax.ShapeDtypeStruct(parts.shape, BF),
        in_specs=[VMEM, VMEM],
        out_specs=VMEM,
        compiler_params=grant(4),
    )(parts, base)


def high_low(x):
    high = x.astype(BF).astype(F32)
    return high, x - high


def feed_kernel(t_ref, r_ref, gain_ref, branch_ref, mix_ref, gate_ref, up_ref, o_ref):
    resid = r_ref[...].reshape(ALL, COLS)
    wide = resid.astype(F32)
    gained = (wide * my_columns(gain_ref, t_ref)).astype(BF)
    for half, w in enumerate((gate_ref, up_ref)):
        for j in range(4):
            part = mm(gained, w[:, j * 128 : (j + 1) * 128]).astype(BF).reshape(EP, ROWS, 128)
            at = ROUTED + (half * 4 + j) * ROWS
            o_ref[:, at : at + ROWS, :] = part
    square_high, square_low = high_low(wide * wide)
    ones = jnp.ones((8, COLS), BF)
    squares = mm_nt(ones, square_high.astype(BF)) + mm_nt(ones, square_low.astype(BF))
    branch = mm_nt(jnp.broadcast_to(my_columns(branch_ref, t_ref), (8, COLS)), gained)
    sq_high, sq_low = high_low(squares)
    br_high, br_low = high_low(branch)
    line = lax.broadcasted_iota(I32, (8, ALL), 0)
    side = jnp.where(line == 0, sq_high, jnp.where(line == 1, sq_low, jnp.where(line == 2, br_high, br_low)))
    me = t_ref[1]
    at = lax.broadcasted_iota(I32, (8 * EP, ALL), 0)
    token = lax.broadcasted_iota(I32, (8 * EP, ALL), 1)
    quarter = at % 8
    mine = (token == (at // 8) * ROWS + 2 * me + quarter // 2) & (quarter < 4)
    own = mm((mine & (quarter % 2 == 0)).astype(F32).astype(BF), resid[:, :128])
    own = own + mm((mine & (quarter % 2 == 1)).astype(F32).astype(BF), resid[:, 128:])
    for g in range(EP):
        tile = g // 4
        block = jnp.concatenate(
            [side[:, tile * 128 : (tile + 1) * 128], own[g * 8 : (g + 1) * 8]], axis=0
        )
        o_ref[g, SIDE:PACKED, :] = block.astype(BF)
    half_rows = CAP * EP // 2
    line = lax.broadcasted_iota(I32, (half_rows, 2 * 128), 0)
    base = (line // CAP) * 128 + line % CAP
    group = lax.broadcasted_iota(I32, (1, 2 * 128), 1) // ROWS
    for half in range(2):
        tiles = []
        for tile in (2 * half, 2 * half + 1):
            tiles.append(sum(mix_ref[4 * tile + i, ROWS:, :].astype(F32) for i in range(4)))
        codes = jnp.concatenate(tiles, axis=1).astype(I32)
        first = codes[0:1] + group * 128 - base
        second = codes[1:2] + group * 128 - base
        source = resid[half * 256 : (half + 1) * 256]
        for x in range(EP):
            member = (first == x * 8) | (second == x * 8)
            picked = mm(jnp.where(member, 1.0, 0.0).astype(BF), source).astype(BF)
            for h in range(2):
                at = h * CAP * EP + half * half_rows
                o_ref[x, at : at + half_rows, :] = picked[:, h * 128 : (h + 1) * 128]


def feed(me, resid, gain, branch, mix, gate, up):
    return pl.pallas_call(
        feed_kernel,
        out_shape=jax.ShapeDtypeStruct((EP, PACKED, 128), BF),
        in_specs=[SMEM] + [VMEM] * 6,
        out_specs=VMEM,
        compiler_params=grant(14),
    )(me, resid, gain, branch, mix, gate, up)


def hidden_kernel(e_ref, p_ref, o_ref, b_ref, kept_ref, kept):
    def total(at, size):
        value = p_ref[0, at : at + size, :].astype(F32)
        for e in range(1, EP):
            value = value + p_ref[e, at : at + size, :].astype(F32)
        return value

    side = total(SIDE, 16)
    lane = lax.broadcasted_iota(I32, (ROWS, 128), 1)
    row = lax.broadcasted_iota(I32, (ROWS, 128), 0)
    mine = lane == (e_ref[0] % 4) * ROWS + row
    squares = jnp.sum(jnp.where(mine, side[0:1] + side[1:2], 0.0), axis=1, keepdims=True)
    branch = jnp.sum(jnp.where(mine, side[2:3] + side[3:4], 0.0), axis=1, keepdims=True)
    scale = lax.rsqrt(squares / WIDTH + EPS)
    for e in range(EP):
        rows = p_ref[e, SIDE:PACKED, :].astype(F32)
        for r in range(2):
            at = r * CHUNKS + 2 * e
            kept[at : at + 2, :] = rows[8 + 2 * r : 10 + 2 * r]
    kept_ref[...] = kept[...].astype(BF)
    b_ref[...] = jnp.broadcast_to(jax.nn.sigmoid(branch * scale), (ROWS, 128))
    for j in range(4):
        gate = total(ROUTED + j * ROWS, ROWS) * scale
        up = total(ROUTED + (4 + j) * ROWS, ROWS) * scale
        value = (gate * jax.nn.sigmoid(gate) * up).astype(BF)
        for e in range(EP):
            o_ref[e, :, j * 128 : (j + 1) * 128] = value


def hidden_units(me, packed):
    return pl.pallas_call(
        hidden_kernel,
        out_shape=(
            jax.ShapeDtypeStruct((EP, ROWS, UNITS), BF),
            jax.ShapeDtypeStruct((ROWS, 128), F32),
            jax.ShapeDtypeStruct((2 * CHUNKS, 128), BF),
        ),
        in_specs=[SMEM, VMEM],
        out_specs=(VMEM,) * 3,
        scratch_shapes=[pltpu.VMEM((2 * CHUNKS, 128), F32)],
        compiler_params=grant(8),
    )(me, packed)


K_STEPS, N_STEPS = 8, 8
PER_STEP = EP // K_STEPS
DEEP = WIDTH // K_STEPS
LANES = WIDTH // N_STEPS


def expert_kernel(
    x_ref, gain_ref, gate_hbm, up_hbm, down_hbm, dense_hbm, o_ref, dense_ref, gate_ref, up_ref, down_ref, turned, done,
):
    slots = CAP * EP
    gates, ups, downs = [], [], []
    for i in range(K_STEPS):
        part = pl.ds(i * DEEP, DEEP)
        gates.append(pltpu.make_async_copy(gate_hbm.at[0, part, :], gate_ref.at[part, :], done.at[0, i]))
        ups.append(pltpu.make_async_copy(up_hbm.at[0, part, :], up_ref.at[part, :], done.at[1, i]))
    for i in range(N_STEPS):
        part = pl.ds(i * LANES, LANES)
        downs.append(pltpu.make_async_copy(down_hbm.at[0, :, part], down_ref.at[:, part], done.at[2, i]))
    dense = pltpu.make_async_copy(dense_hbm, dense_ref, done.at[3, 0])
    for i in range(K_STEPS):
        gates[i].start()
        ups[i].start()
    for move in downs:
        move.start()
    dense.start()
    squares = jnp.zeros((slots, 128), F32)
    gate = jnp.zeros((slots, COLS), F32)
    up = jnp.zeros((slots, COLS), F32)
    for i in range(K_STEPS):
        pieces = []
        for e in range(i * PER_STEP, (i + 1) * PER_STEP):
            for h in range(2):
                x = x_ref[e, h * slots : (h + 1) * slots, :].astype(F32)
                squares += x * x
                at = (2 * e + h) * 128
                pieces.append((x * gain_ref[:, at : at + 128]).astype(BF))
        x = jnp.concatenate(pieces, axis=1)
        gates[i].wait()
        ups[i].wait()
        gate += mm(x, gate_ref[i * DEEP : (i + 1) * DEEP, :])
        up += mm(x, up_ref[i * DEEP : (i + 1) * DEEP, :])
    scale = lax.rsqrt(jnp.sum(squares, axis=1, keepdims=True) / WIDTH + EPS)
    gate = gate * scale
    hidden = (gate * jax.nn.sigmoid(gate) * (up * scale)).astype(BF)
    for i in range(N_STEPS):
        downs[i].wait()
        out = mm(hidden, down_ref[:, i * LANES : (i + 1) * LANES])
        for c in range(LANES // 128):
            turned[pl.ds(i * (LANES // 128) + c, slots, stride=CHUNKS), :] = out[:, c * 128 : (c + 1) * 128]
    for g in range(EP):
        o_ref[g, :BACK, :] = turned[g * BACK : (g + 1) * BACK, :].astype(BF)
    dense.wait()


def expert(packed, gain, gate, up, down_w, dense_w):
    return pl.pallas_call(
        expert_kernel,
        out_shape=(
            jax.ShapeDtypeStruct((EP, RETURN, 128), BF),
            jax.ShapeDtypeStruct(dense_w.shape, BF),
        ),
        in_specs=[VMEM, VMEM, HBM, HBM, HBM, HBM],
        out_specs=(VMEM, VMEM),
        scratch_shapes=[
            pltpu.VMEM((WIDTH, COLS), BF),
            pltpu.VMEM((WIDTH, COLS), BF),
            pltpu.VMEM((COLS, WIDTH), BF),
            pltpu.VMEM((CAP * EP * CHUNKS, 128), F32),
            pltpu.SemaphoreType.DMA((4, 8)),
        ],
        compiler_params=grant(14),
    )(packed, gain, in_hbm(gate), in_hbm(up), in_hbm(down_w), in_hbm(dense_w))


def down_kernel(h_ref, w_ref, _, o_ref):
    out = mm(h_ref[...].reshape(ALL, UNITS), w_ref[...]).astype(BF)
    for h in range(2):
        o_ref[:, h * ROWS : (h + 1) * ROWS, :] = out[:, h * 128 : (h + 1) * 128].reshape(EP, ROWS, 128)


def down(hidden, w, buffer):
    whole = lambda *shape: pl.BlockSpec(shape, lambda i: (0,) * len(shape))
    return pl.pallas_call(
        down_kernel,
        grid=(1,),
        out_shape=jax.ShapeDtypeStruct((EP, RETURN, 128), BF),
        in_specs=[whole(EP, ROWS, UNITS), whole(UNITS, COLS), pl.BlockSpec(memory_space=pl.ANY)],
        out_specs=pl.BlockSpec((EP, 2 * ROWS, 128), lambda i: (0, BACK // (2 * ROWS), 0)),
        input_output_aliases={2: 0},
        compiler_params=grant(6),
    )(hidden, w, buffer)


def gather_kernel(table_ref, branch_ref, r_ref, o_ref, dense):
    for c in range(CHUNKS):
        at = BACK + (c % 2) * ROWS
        dense[c * ROWS : (c + 1) * ROWS, :] = r_ref[c // 2, at : at + ROWS, :].astype(F32)
    for r in range(ROWS):
        total = branch_ref[r : r + 1, :] * dense[pl.ds(r, CHUNKS, stride=ROWS), :]
        for k in range(2):
            code = table_ref[k, r].astype(I32)
            at = pl.multiple_of((code % 8) * CHUNKS, CHUNKS)
            total = total + table_ref[2 + k, r] * r_ref[code // 8, pl.ds(at, CHUNKS), :].astype(F32)
        o_ref[r // 2, (r % 2) * CHUNKS : (r % 2 + 1) * CHUNKS, :] = total.astype(BF)


def gather(table, branch, returned):
    return pl.pallas_call(
        gather_kernel,
        out_shape=jax.ShapeDtypeStruct((TP, 2 * CHUNKS, 128), BF),
        in_specs=[SMEM, VMEM, VMEM],
        out_specs=VMEM,
        scratch_shapes=[pltpu.VMEM((CHUNKS * ROWS, 128), F32)],
        compiler_params=grant(6),
    )(table, branch, returned)


def on_device(
    tokens,
    state_matrix,
    state_norm,
    state_max,
    mixer_gain,
    w_query,
    w_key,
    w_value,
    w_outgate,
    w_ingate,
    w_forget,
    forget_bias,
    w_proj,
    ffn_gain,
    w_branch,
    routes,
    route_weight,
    expert_gate,
    expert_up,
    expert_down,
    dense_gate,
    dense_up,
    dense_down,
):
    me = jnp.stack([lax.axis_index("ep"), lax.axis_index("tp")]).astype(I32)
    token_cols = swap(cut(tokens), "ep")
    own = prepare(
        me, tokens, mixer_gain[None], w_ingate.T, w_forget.T, forget_bias[None], state_max.T, state_norm,
        routes.T, route_weight.T, state_matrix,
    )
    gains = (mixer_gain[None], ffn_gain[None], w_branch[None])
    scale, write, new_max, extra, table, norm, old = own
    (token_cols, scale, write, extra, norm, old, gains, me) = lax.optimization_barrier(
        (token_cols, scale, write, extra, norm, old, gains, me)
    )
    partial, token_block = heads(me, token_cols, gains[0], (w_query, w_key, w_value, w_outgate))
    parts = swap(partial, "ep")
    mixed, new_norm, new_matrix = cell(parts, scale, write, extra, norm, old)
    mixed_all = swap(mixed, "ep")

    spread_out = mm(mixed_all[:, :ROWS].reshape(ALL, HEAD), w_proj).astype(BF).reshape(TP, ROWS, COLS)
    resid = swap(settle(swap(spread_out, "tp"), token_block), "tp")

    arrived = swap(feed(me, resid, gains[1], gains[2], mixed_all, dense_gate, dense_up), "ep")
    hidden, branch, kept = hidden_units(me, arrived)
    hidden_all = swap(hidden, "ep")

    _, arrived = lax.optimization_barrier((hidden, arrived))
    buffer, down_w = expert(arrived, gains[1], expert_gate, expert_up, expert_down, dense_down)
    hidden_all, buffer, down_w, branch, kept, new_max, new_norm, table = lax.optimization_barrier(
        (hidden_all, buffer, down_w, branch, kept, new_max, new_norm, table)
    )

    returned = swap(down(hidden_all, down_w, buffer), "ep")
    parts = swap(gather(table, branch, returned), "tp")
    layer_out = swap(settle(parts, kept), "tp").reshape(ROWS, WIDTH)
    new_max = new_max.T
    return (layer_out, new_matrix, new_norm[:, None], new_max)


def solution(mesh):
    in_specs = (
        P("ep", None),
        P("ep", "tp", None, None),
        P("ep", "tp", None),
        P("ep", "tp"),
        P(),
        P("ep", "tp"),
        P("ep", "tp"),
        P("ep", "tp"),
        P("ep", "tp"),
        P(),
        P(),
        P(),
        P("tp", "ep"),
        P(),
        P(),
        P("ep", None),
        P("ep", None),
        P("ep", None, "tp"),
        P("ep", None, "tp"),
        P("ep", "tp", None),
        P("ep", "tp"),
        P("ep", "tp"),
        P("tp", "ep"),
    )
    out_specs = (P("ep", None), P("ep", "tp", None, None), P("ep", "tp", None), P("ep", "tp"))
    return jax.shard_map(
        on_device, mesh=mesh, in_specs=in_specs, out_specs=out_specs, check_vma=False
    )
```

```python
import jax
import jax.numpy as jnp
from jax import lax
from jax.experimental import pallas as pl
from jax.experimental.pallas import tpu as pltpu
from jax.sharding import PartitionSpec as P

EPS = 1e-06
BF = jnp.bfloat16
F32 = jnp.float32
I32 = jnp.int32
EP, TP = 16, 16
ROWS, WIDTH, COLS, HEAD, UNITS, CAP = 32, 4096, 256, 128, 512, 6
ALL = ROWS * EP
ROUTED = CAP * EP
SIDE = ROUTED + 8 * ROWS
PACKED = SIDE + 16
CHUNKS = WIDTH // 128
BACK = CAP * EP
RETURN = BACK + 2 * ROWS
def in_hbm(x):
    return pltpu.with_memory_space_constraint(x, pltpu.HBM)


def grant(mib):
    return pltpu.CompilerParams(vmem_limit_bytes=mib * 1024 * 1024)


VMEM = pl.BlockSpec(memory_space=pltpu.VMEM)
SMEM = pl.BlockSpec(memory_space=pltpu.SMEM)
HBM = pl.BlockSpec(memory_space=pltpu.HBM)


def swap(parts, axis):
    return lax.all_to_all(parts, axis, 0, 0, tiled=True)


def copies(shard, axis):
    return swap(jnp.broadcast_to(shard[None], (lax.axis_size(axis), *shard.shape)), axis)


def mm(a, b):
    return jnp.dot(a, b, preferred_element_type=F32)


def mm_nt(a, b):
    return lax.dot_general(a, b, (((1,), (1,)), ((), ())), preferred_element_type=F32)


def cut_kernel(x_hbm, o_hbm, x_ref, o_ref, done):
    half = ROWS // 2
    rows = [pl.ds(i * half, half) for i in range(2)]
    into = [pltpu.make_async_copy(x_hbm.at[r], x_ref.at[r], done.at[0, i]) for i, r in enumerate(rows)]
    back = [pltpu.make_async_copy(o_ref.at[:, r], o_hbm.at[:, r], done.at[1, i]) for i, r in enumerate(rows)]
    for move in into:
        move.start()
    for i in range(2):
        into[i].wait()
        for e in range(EP):
            o_ref[e, i * half : (i + 1) * half] = x_ref[i * half : (i + 1) * half, e * COLS : (e + 1) * COLS]
        back[i].start()
    for move in back:
        move.wait()


def cut(tokens):
    return pl.pallas_call(
        cut_kernel,
        out_shape=jax.ShapeDtypeStruct((EP, ROWS, COLS), BF),
        in_specs=[HBM],
        out_specs=HBM,
        scratch_shapes=[
            pltpu.VMEM((ROWS, WIDTH), BF), pltpu.VMEM((EP, ROWS, COLS), BF), pltpu.SemaphoreType.DMA((2, 2)),
        ],
        compiler_params=grant(2),
    )(in_hbm(tokens))


def prepare_kernel(
    me_ref, *refs,
):
    sources, outs, scratch = refs[:10], refs[10:17], refs[17:27]
    done = refs[27]
    moves = [pltpu.make_async_copy(a, b, done.at[i]) for i, (a, b) in enumerate(zip(sources, scratch))]
    for move in moves:
        move.start()
    x_ref, gain_ref, in_ref, forget_ref, bias_ref, max_ref, norm_ref, route_ref, weight_ref, state_ref = scratch
    scale_ref, write_ref, new_max_ref, extra_ref, table_ref, old_norm_ref, old_ref = outs
    for move in moves[:-1]:
        move.wait()
    wide = x_ref[...].astype(F32)
    scale = lax.rsqrt(jnp.sum(wide * wide, axis=1, keepdims=True) / WIDTH + EPS)
    scale_ref[...] = jnp.broadcast_to(scale, (ROWS, HEAD))
    normed = (wide * scale * gain_ref[...]).astype(BF)
    head = lax.broadcasted_iota(I32, (ROWS, TP), 1) == me_ref[1]
    pick = lambda x: jnp.sum(jnp.where(head, x, 0.0), axis=1, keepdims=True)
    row = lax.broadcasted_iota(I32, (ROWS, ROWS), 0)
    lane = lax.broadcasted_iota(I32, (ROWS, ROWS), 1)
    upright = lambda x: jnp.sum(jnp.where(lane == row, x, jnp.zeros_like(x)), axis=1, keepdims=True)
    flat = lambda x: jnp.sum(jnp.where(lane == row, x, jnp.zeros_like(x)), axis=0, keepdims=True)
    gate_in = pick(mm_nt(normed, in_ref[...]))
    gate_forget = pick(mm_nt(normed, forget_ref[...]) + bias_ref[...])
    old_max = upright(max_ref[...])
    log_keep = jnp.minimum(gate_forget, 0.0) - jnp.log1p(jnp.exp(-jnp.abs(gate_forget)))
    new_max = jnp.maximum(log_keep + old_max, gate_in)
    new_max_ref[...] = flat(new_max)
    keep = jnp.broadcast_to(jnp.exp(log_keep + old_max - new_max), (ROWS, HEAD))
    write_ref[...] = jnp.broadcast_to(jnp.exp(gate_in - new_max), (ROWS, HEAD))
    old_norm_ref[...] = keep * norm_ref[...].reshape(ROWS, HEAD)

    place = lax.broadcasted_iota(I32, (ROWS, 128), 1) == (me_ref[0] % 4) * ROWS + lax.broadcasted_iota(
        I32, (ROWS, 128), 0
    )
    across = [route_ref[k : k + 1, :] for k in range(2)]
    column = [upright(x) for x in across]
    lines = []
    for k in range(2):
        same = (across[0] == column[k]).astype(I32) + (across[1] == column[k]).astype(I32)
        slot = jnp.sum(jnp.where(lane < row, same, 0), axis=1, keepdims=True)
        code = column[k] * 8 + slot
        table_ref[k : k + 1, :] = flat(code).astype(F32)
        lines.append(jnp.sum(jnp.where(place, code, 0), axis=0, keepdims=True))
    lines.append(jnp.zeros((6, 128), I32))
    extra_ref[...] = jnp.concatenate(lines, axis=0).astype(F32).astype(BF)
    weight = weight_ref[...]
    table_ref[2:4, :] = weight / jnp.sum(weight, axis=0, keepdims=True)
    moves[-1].wait()
    for r in range(ROWS):
        old_ref[r] = keep[r : r + 1] * state_ref[r, 0]


def prepare(me, *sources):
    wide = jax.ShapeDtypeStruct((ROWS, HEAD), F32)
    return pl.pallas_call(
        prepare_kernel,
        out_shape=(
            wide, wide, jax.ShapeDtypeStruct((1, ROWS), F32), jax.ShapeDtypeStruct((8, HEAD), BF),
            jax.ShapeDtypeStruct((4, ROWS), F32), wide, jax.ShapeDtypeStruct((ROWS, HEAD, HEAD), F32),
        ),
        in_specs=[SMEM] + [HBM] * 10,
        out_specs=(VMEM,) * 7,
        scratch_shapes=[pltpu.VMEM(x.shape, x.dtype) for x in sources] + [pltpu.SemaphoreType.DMA((10,))],
        compiler_params=grant(12),
    )(me, *[in_hbm(x) for x in sources])


def my_columns(ref, me_ref):
    return ref[:, pl.ds(pl.multiple_of(me_ref[0] * COLS, COLS), COLS)]


def heads_kernel(me_ref, x_ref, gain_ref, q_ref, k_ref, v_ref, g_ref, o_ref, mine_ref):
    x = (x_ref[...].reshape(ALL, COLS).astype(F32) * my_columns(gain_ref, me_ref)).astype(BF)
    for i, w in enumerate((q_ref, k_ref, v_ref, g_ref)):
        o_ref[:, :, i * HEAD : (i + 1) * HEAD] = mm(x, w[...]).astype(BF).reshape(EP, ROWS, HEAD)
    mine_ref[...] = x_ref[me_ref[1]]


def heads(me, token_cols, gain, ws):
    return pl.pallas_call(
        heads_kernel,
        out_shape=(
            jax.ShapeDtypeStruct((EP, ROWS, 4 * HEAD), BF),
            jax.ShapeDtypeStruct((ROWS, COLS), BF),
        ),
        in_specs=[SMEM] + [VMEM] * 6,
        out_specs=(VMEM, VMEM),
        compiler_params=grant(6),
    )(me, token_cols, gain, *ws)


STEP = 8


def cell_kernel(p_ref, scale_ref, write_ref, extra_ref, norm_ref, old_ref, mixed_ref, new_norm_ref, new_hbm, numer, new_ref, done):
    proj = []
    for i in range(4):
        lanes = slice(i * HEAD, (i + 1) * HEAD)
        total = p_ref[0, :, lanes].astype(F32)
        for e in range(1, EP):
            total = total + p_ref[e, :, lanes].astype(F32)
        proj.append(total * scale_ref[...])
    query, key, value, outgate = proj
    wkey = write_ref[...] * (key * HEAD ** (-0.5))
    new_norm = norm_ref[...] + wkey
    new_norm_ref[...] = new_norm
    moves = []
    for step in range(ROWS // STEP):
        here = slice(step * STEP, (step + 1) * STEP)
        query_t, wkey_t = query[here].T, wkey[here].T
        for j in range(STEP):
            row = step * STEP + j
            new = old_ref[row] + wkey_t[:, j : j + 1] * value[row : row + 1]
            new_ref[row, 0] = new
            numer[row : row + 1, :] = jnp.sum(query_t[:, j : j + 1] * new, axis=0, keepdims=True)
        moves.append(pltpu.make_async_copy(new_ref.at[pl.ds(step * STEP, STEP)], new_hbm.at[pl.ds(step * STEP, STEP)], done.at[step]))
        moves[-1].start()
    denom = jnp.sum(query * new_norm, axis=1, keepdims=True)
    out = numer[...] / jnp.maximum(jnp.abs(denom), 1.0)
    mixed = (jax.nn.sigmoid(outgate) * out).astype(BF)
    extra = extra_ref[...]
    for e in range(EP):
        mixed_ref[e, :ROWS] = mixed
        mixed_ref[e, ROWS:] = extra
    for move in moves:
        move.wait()


def cell(parts, scale, write, extra, norm, old):
    return pl.pallas_call(
        cell_kernel,
        out_shape=(
            jax.ShapeDtypeStruct((EP, ROWS + 8, HEAD), BF),
            jax.ShapeDtypeStruct((ROWS, HEAD), F32),
            jax.ShapeDtypeStruct((ROWS, 1, HEAD, HEAD), F32),
        ),
        in_specs=[VMEM] * 6,
        out_specs=(VMEM, VMEM, HBM),
        scratch_shapes=[
            pltpu.VMEM((ROWS, HEAD), F32),
            pltpu.VMEM((ROWS, 1, HEAD, HEAD), F32),
            pltpu.SemaphoreType.DMA((ROWS // STEP,)),
        ],
        compiler_params=grant(8),
    )(parts, scale, write, extra, norm, old)


def settle_kernel(p_ref, base_ref, o_ref):
    total = p_ref[0].astype(F32)
    for t in range(1, TP):
        total = total + p_ref[t].astype(F32)
    out = (base_ref[...].astype(F32) + total).astype(BF)
    for t in range(TP):
        o_ref[t] = out


def settle(parts, base):
    return pl.pallas_call(
        settle_kernel,
        out_shape=jax.ShapeDtypeStruct(parts.shape, BF),
        in_specs=[VMEM, VMEM],
        out_specs=VMEM,
        compiler_params=grant(4),
    )(parts, base)


def high_low(x):
    high = x.astype(BF).astype(F32)
    return high, x - high


def feed_kernel(t_ref, r_ref, gain_ref, branch_ref, mix_ref, gate_ref, up_ref, o_ref):
    resid = r_ref[...].reshape(ALL, COLS)
    wide = resid.astype(F32)
    gained = (wide * my_columns(gain_ref, t_ref)).astype(BF)
    for half, w in enumerate((gate_ref, up_ref)):
        for j in range(4):
            part = mm(gained, w[:, j * 128 : (j + 1) * 128]).astype(BF).reshape(EP, ROWS, 128)
            at = ROUTED + (half * 4 + j) * ROWS
            o_ref[:, at : at + ROWS, :] = part
    square_high, square_low = high_low(wide * wide)
    ones = jnp.ones((8, COLS), BF)
    squares = mm_nt(ones, square_high.astype(BF)) + mm_nt(ones, square_low.astype(BF))
    line = lax.broadcasted_iota(I32, (2 * EP, 128), 0)
    pick = lambda h: jnp.sum(jnp.where(line == 2 * t_ref[0] + h, branch_ref[...].astype(F32), 0.0), axis=0, keepdims=True)
    weights = jnp.concatenate([pick(0), pick(1)], axis=1).astype(BF)
    branch = mm_nt(jnp.broadcast_to(weights, (8, COLS)), gained)
    sq_high, sq_low = high_low(squares)
    br_high, br_low = high_low(branch)
    line = lax.broadcasted_iota(I32, (8, ALL), 0)
    side = jnp.where(line == 0, sq_high, jnp.where(line == 1, sq_low, jnp.where(line == 2, br_high, br_low)))
    at = lax.broadcasted_iota(I32, (8 * EP, ALL), 0)
    token = lax.broadcasted_iota(I32, (8 * EP, ALL), 1)
    quarter = at % 8
    mine = (token == (at // 8) * ROWS + 2 * t_ref[1] + quarter // 2) & (quarter < 4)
    own = mm((mine & (quarter % 2 == 0)).astype(F32).astype(BF), resid[:, :128])
    own = own + mm((mine & (quarter % 2 == 1)).astype(F32).astype(BF), resid[:, 128:])
    for g in range(EP):
        tile = g // 4
        block = jnp.concatenate(
            [side[:, tile * 128 : (tile + 1) * 128], own[g * 8 : (g + 1) * 8]], axis=0
        )
        o_ref[g, SIDE:PACKED, :] = block.astype(BF)
    half_rows = CAP * EP // 2
    line = lax.broadcasted_iota(I32, (half_rows, 2 * 128), 0)
    base = (line // CAP) * 128 + line % CAP
    group = lax.broadcasted_iota(I32, (1, 2 * 128), 1) // ROWS
    for half in range(2):
        tiles = []
        for tile in (2 * half, 2 * half + 1):
            tiles.append(sum(mix_ref[4 * tile + i, ROWS:, :].astype(F32) for i in range(4)))
        codes = jnp.concatenate(tiles, axis=1).astype(I32)
        first = codes[0:1] + group * 128 - base
        second = codes[1:2] + group * 128 - base
        source = jnp.where(t_ref[1] % 2 == 0, wide[:, :128], wide[:, 128:])[half * 256 : (half + 1) * 256].astype(BF)
        for x in range(EP):
            member = (first == x * 8) | (second == x * 8)
            picked = mm(jnp.where(member, 1.0, 0.0).astype(BF), source).astype(BF)
            o_ref[x, half * half_rows : (half + 1) * half_rows, :] = picked


def feed(me, resid, gain, branch, mix, gate, up):
    return pl.pallas_call(
        feed_kernel,
        out_shape=jax.ShapeDtypeStruct((EP, PACKED, 128), BF),
        in_specs=[SMEM] + [VMEM] * 6,
        out_specs=VMEM,
        compiler_params=grant(14),
    )(me, resid, gain, branch, mix, gate, up)


def over_peers(ref, at, size):
    value = ref[0, at : at + size, :].astype(F32)
    for e in range(1, EP):
        value = value + ref[e, at : at + size, :].astype(F32)
    return value


def token_sums(me_ref, side):
    lane = lax.broadcasted_iota(I32, (ROWS, 128), 1)
    row = lax.broadcasted_iota(I32, (ROWS, 128), 0)
    mine = lane == (me_ref[0] % 4) * ROWS + row
    squares = jnp.sum(jnp.where(mine, side[0:1] + side[1:2], 0.0), axis=1, keepdims=True)
    branch = jnp.sum(jnp.where(mine, side[2:3] + side[3:4], 0.0), axis=1, keepdims=True)
    return lax.rsqrt(squares / WIDTH + EPS), branch


def hidden_kernel(me_ref, p_ref, o_ref):
    scale, _ = token_sums(me_ref, over_peers(p_ref, SIDE, 16))
    for j in range(4):
        gate = over_peers(p_ref, ROUTED + j * ROWS, ROWS) * scale
        up = over_peers(p_ref, ROUTED + (4 + j) * ROWS, ROWS) * scale
        value = (gate * jax.nn.sigmoid(gate) * up).astype(BF)
        for e in range(EP):
            o_ref[e, :, j * 128 : (j + 1) * 128] = value


def hidden_units(me, packed):
    return pl.pallas_call(
        hidden_kernel,
        out_shape=jax.ShapeDtypeStruct((EP, ROWS, UNITS), BF),
        in_specs=[SMEM, VMEM],
        out_specs=VMEM,
        compiler_params=grant(8),
    )(me, packed)


def sides_kernel(me_ref, p_ref, b_ref, kept_ref, kept):
    scale, branch = token_sums(me_ref, over_peers(p_ref, SIDE, 16))
    b_ref[...] = jnp.broadcast_to(jax.nn.sigmoid(branch * scale), (ROWS, 128))
    for e in range(EP):
        rows = p_ref[e, SIDE:PACKED, :].astype(F32)
        for q in range(4):
            kept[q * EP + e : q * EP + e + 1, :] = rows[8 + q : 9 + q]
    kept_ref[...] = kept[...].astype(BF)


def sides(me, packed):
    return pl.pallas_call(
        sides_kernel,
        out_shape=(
            jax.ShapeDtypeStruct((ROWS, 128), F32),
            jax.ShapeDtypeStruct((2 * CHUNKS, 128), BF),
        ),
        in_specs=[SMEM, VMEM],
        out_specs=(VMEM, VMEM),
        scratch_shapes=[pltpu.VMEM((2 * CHUNKS, 128), F32)],
        compiler_params=grant(4),
    )(me, packed)


K_STEPS, N_STEPS = 8, 8
PER_STEP = EP // K_STEPS
DEEP = WIDTH // K_STEPS
LANES = WIDTH // N_STEPS


def expert_kernel(
    me_ref, x_ref, y_ref, gain_ref, gate_hbm, up_hbm, down_hbm, o_ref, send_ref, gate_ref, up_ref, down_ref, turned, done,
):
    slots = CAP * EP
    core = me_ref[1] % 2
    gates, ups, downs = [], [], []
    for i in range(K_STEPS):
        part = pl.ds(i * DEEP, DEEP)
        gates.append(pltpu.make_async_copy(gate_hbm.at[0, part, :], gate_ref.at[part, :], done.at[0, i]))
        ups.append(pltpu.make_async_copy(up_hbm.at[0, part, :], up_ref.at[part, :], done.at[1, i]))
    for i in range(N_STEPS):
        part = pl.ds(i * LANES, LANES)
        downs.append(pltpu.make_async_copy(down_hbm.at[0, :, part], down_ref.at[:, part], done.at[2, i]))
    for i in range(K_STEPS):
        gates[i].start()
        ups[i].start()
    for move in downs:
        move.start()
    squares = jnp.zeros((slots, 128), F32)
    gate = jnp.zeros((slots, COLS), F32)
    up = jnp.zeros((slots, COLS), F32)
    for i in range(K_STEPS):
        pieces = []
        for e in range(i * PER_STEP, (i + 1) * PER_STEP):
            for h in range(2):
                x = jnp.where(core == h, x_ref[e, :ROUTED, :].astype(F32), y_ref[e].astype(F32))
                squares += x * x
                at = (2 * e + h) * 128
                pieces.append((x * gain_ref[:, at : at + 128]).astype(BF))
        x = jnp.concatenate(pieces, axis=1)
        gates[i].wait()
        ups[i].wait()
        gate += mm(x, gate_ref[i * DEEP : (i + 1) * DEEP, :])
        up += mm(x, up_ref[i * DEEP : (i + 1) * DEEP, :])
    scale = lax.rsqrt(jnp.sum(squares, axis=1, keepdims=True) / WIDTH + EPS)
    gate = gate * scale
    hidden = (gate * jax.nn.sigmoid(gate) * (up * scale)).astype(BF)
    for i in range(N_STEPS):
        downs[i].wait()
        out = mm(hidden, down_ref[:, i * LANES : (i + 1) * LANES])
        for c in range(LANES // 128):
            chunk = i * (LANES // 128) + c
            at = (chunk % 2) * slots * EP + chunk // 2
            turned[pl.ds(at, slots, stride=EP), :] = out[:, c * 128 : (c + 1) * 128]
    for g in range(EP):
        mine = pl.multiple_of(core * slots * EP + g * BACK, BACK)
        other = pl.multiple_of((1 - core) * slots * EP + g * BACK, BACK)
        o_ref[g] = turned[pl.ds(mine, BACK), :].astype(BF)
        send_ref[g] = turned[pl.ds(other, BACK), :].astype(BF)


def expert(me, packed, other, gain, gate, up, down_w):
    rows = jax.ShapeDtypeStruct((EP, BACK, 128), BF)
    return pl.pallas_call(
        expert_kernel,
        out_shape=(rows, rows),
        in_specs=[SMEM, VMEM, VMEM, VMEM, HBM, HBM, HBM],
        out_specs=(VMEM, VMEM),
        scratch_shapes=[
            pltpu.VMEM((WIDTH, COLS), BF),
            pltpu.VMEM((WIDTH, COLS), BF),
            pltpu.VMEM((COLS, WIDTH), BF),
            pltpu.VMEM((CAP * EP * CHUNKS, 128), F32),
            pltpu.SemaphoreType.DMA((3, 8)),
        ],
        compiler_params=grant(16),
    )(me, packed, other, gain, in_hbm(gate), in_hbm(up), in_hbm(down_w))


def down_kernel(h_ref, w_ref, x_ref, y_ref, o_ref):
    for g in range(EP):
        o_ref[g, :BACK, :] = (x_ref[g].astype(F32) + y_ref[g].astype(F32)).astype(BF)
    out = mm(h_ref[...].reshape(ALL, UNITS), w_ref[...]).astype(BF)
    for h in range(2):
        at = BACK + h * ROWS
        o_ref[:, at : at + ROWS, :] = out[:, h * 128 : (h + 1) * 128].reshape(EP, ROWS, 128)


def down(hidden, w, rows, more):
    return pl.pallas_call(
        down_kernel,
        out_shape=jax.ShapeDtypeStruct((EP, RETURN, 128), BF),
        in_specs=[VMEM] * 4,
        out_specs=VMEM,
        compiler_params=grant(6),
    )(hidden, w, rows, more)


def gather_kernel(me_ref, table_ref, branch_ref, r_ref, o_ref, dense):
    for h in range(2):
        for e in range(EP):
            at = (h * EP + e) * ROWS
            dense[at : at + ROWS, :] = r_ref[e, BACK + h * ROWS : BACK + (h + 1) * ROWS, :].astype(F32)
    mine = lax.broadcasted_iota(I32, (CHUNKS, 128), 0) // EP == me_ref[1] % 2
    for r in range(ROWS):
        total = jnp.zeros((EP, 128), F32)
        for k in range(2):
            code = table_ref[k, r].astype(I32)
            at = pl.multiple_of((code % 8) * EP, EP)
            total = total + table_ref[2 + k, r] * r_ref[code // 8, pl.ds(at, EP), :].astype(F32)
        total = jnp.where(mine, jnp.concatenate([total, total], axis=0), 0.0)
        total = total + branch_ref[r : r + 1, :] * dense[pl.ds(r, CHUNKS, stride=ROWS), :]
        o_ref[r // 2, (r % 2) * CHUNKS : (r % 2 + 1) * CHUNKS, :] = total.astype(BF)


def gather(me, table, branch, returned):
    return pl.pallas_call(
        gather_kernel,
        out_shape=jax.ShapeDtypeStruct((TP, 2 * CHUNKS, 128), BF),
        in_specs=[SMEM, SMEM, VMEM, VMEM],
        out_specs=VMEM,
        scratch_shapes=[pltpu.VMEM((CHUNKS * ROWS, 128), F32)],
        compiler_params=grant(6),
    )(me, table, branch, returned)


def finish_kernel(p_ref, kept_ref, o_ref, turned):
    total = p_ref[0].astype(F32)
    for t in range(1, TP):
        total = total + p_ref[t].astype(F32)
    total = total + kept_ref[...].astype(F32)
    for r in range(2):
        for h in range(2):
            at = r * CHUNKS + h * EP
            turned[pl.ds(r * CHUNKS + h, EP, stride=2), :] = total[at : at + EP]
    out = turned[...].astype(BF)
    for t in range(TP):
        o_ref[t] = out


def finish(parts, kept):
    return pl.pallas_call(
        finish_kernel,
        out_shape=jax.ShapeDtypeStruct(parts.shape, BF),
        in_specs=[VMEM, VMEM],
        out_specs=VMEM,
        scratch_shapes=[pltpu.VMEM((2 * CHUNKS, 128), F32)],
        compiler_params=grant(4),
    )(parts, kept)


def on_device(
    tokens,
    state_matrix,
    state_norm,
    state_max,
    mixer_gain,
    w_query,
    w_key,
    w_value,
    w_outgate,
    w_ingate,
    w_forget,
    forget_bias,
    w_proj,
    ffn_gain,
    w_branch,
    routes,
    route_weight,
    expert_gate,
    expert_up,
    expert_down,
    dense_gate,
    dense_up,
    dense_down,
):
    me = jnp.stack([lax.axis_index("ep"), lax.axis_index("tp")]).astype(I32)
    token_cols = swap(cut(tokens), "ep")
    own = prepare(
        me, tokens, mixer_gain[None], w_ingate.T, w_forget.T, forget_bias[None], state_max.T, state_norm,
        routes.T, route_weight.T, state_matrix,
    )
    gains = (mixer_gain[None], ffn_gain[None], w_branch.reshape(2 * EP, 128))
    scale, write, new_max, extra, table, norm, old = own
    (token_cols, scale, write, extra, norm, old, gains, me) = lax.optimization_barrier(
        (token_cols, scale, write, extra, norm, old, gains, me)
    )
    partial, token_block = heads(me, token_cols, gains[0], (w_query, w_key, w_value, w_outgate))
    parts = swap(partial, "ep")
    mixed, new_norm, new_matrix = cell(parts, scale, write, extra, norm, old)
    mixed_all = swap(mixed, "ep")

    spread_out = mm(mixed_all[:, :ROWS].reshape(ALL, HEAD), w_proj).astype(BF).reshape(TP, ROWS, COLS)
    resid = swap(settle(swap(spread_out, "tp"), token_block), "tp")

    packed = swap(feed(me, resid, gains[1], gains[2], mixed_all, dense_gate, dense_up), "ep")
    cores = [(t, t ^ 1) for t in range(TP)]
    other = lax.ppermute(packed[:, :ROUTED], "tp", cores)
    hidden = hidden_units(me, packed)
    hidden_all = swap(hidden, "ep")

    _, packed, other = lax.optimization_barrier((hidden, packed, other))
    branch, kept = sides(me, packed)
    rows_out, rows_sent = expert(me, packed, other, gains[1], expert_gate, expert_up, expert_down)
    more = lax.ppermute(rows_sent, "tp", cores)
    hidden_all, rows_out, more, branch, kept, new_max, new_norm, table = lax.optimization_barrier(
        (hidden_all, rows_out, more, branch, kept, new_max, new_norm, table)
    )

    returned = swap(down(hidden_all, dense_down, rows_out, more), "ep")
    parts = swap(gather(me, table, branch, returned), "tp")
    layer_out = swap(finish(parts, kept), "tp").reshape(ROWS, WIDTH)
    new_max = new_max.T
    return (layer_out, new_matrix, new_norm[:, None], new_max)


def solution(mesh):
    in_specs = (
        P("ep", None),
        P("ep", "tp", None, None),
        P("ep", "tp", None),
        P("ep", "tp"),
        P(),
        P("ep", "tp"),
        P("ep", "tp"),
        P("ep", "tp"),
        P("ep", "tp"),
        P(),
        P(),
        P(),
        P("tp", "ep"),
        P(),
        P(),
        P("ep", None),
        P("ep", None),
        P("ep", None, "tp"),
        P("ep", None, "tp"),
        P("ep", "tp", None),
        P("ep", "tp"),
        P("ep", "tp"),
        P("tp", "ep"),
    )
    out_specs = (P("ep", None), P("ep", "tp", None, None), P("ep", "tp", None), P("ep", "tp"))
    return jax.shard_map(
        on_device, mesh=mesh, in_specs=in_specs, out_specs=out_specs, check_vma=False
    )
```

```python
import jax
import jax.numpy as jnp
from jax import lax
from jax.experimental import pallas as pl
from jax.experimental.pallas import tpu as pltpu
from jax.sharding import PartitionSpec as P

EPS = 1e-06
BF = jnp.bfloat16
F32 = jnp.float32
I32 = jnp.int32
EP, TP = 16, 16
ROWS, WIDTH, COLS, HEAD, UNITS, CAP = 32, 4096, 256, 128, 512, 6
ALL = ROWS * EP
ROUTED = CAP * EP
SIDE = ROUTED + 8 * ROWS
PACKED = SIDE + 16
CHUNKS = WIDTH // 128
BACK = CAP * EP
RETURN = BACK + 2 * ROWS
def in_hbm(x):
    return pltpu.with_memory_space_constraint(x, pltpu.HBM)


def in_vmem(x):
    return pltpu.with_memory_space_constraint(x, pltpu.VMEM)


def grant(mib):
    return pltpu.CompilerParams(vmem_limit_bytes=mib * 1024 * 1024)


VMEM = pl.BlockSpec(memory_space=pltpu.VMEM)
SMEM = pl.BlockSpec(memory_space=pltpu.SMEM)
HBM = pl.BlockSpec(memory_space=pltpu.HBM)


def swap(parts, axis):
    return lax.all_to_all(parts, axis, 0, 0, tiled=True)


CHIPS = TP // 2
ALONG_Z = [[2 * z + core for z in range(CHIPS)] for core in range(2)]
CORES = [(t, t ^ 1) for t in range(TP)]


def swap_z(parts):
    return lax.all_to_all(parts, "tp", 0, 0, tiled=True, axis_index_groups=ALONG_Z)


def from_core(x):
    return lax.ppermute(x, "tp", CORES)


def mm(a, b):
    return jnp.dot(a, b, preferred_element_type=F32)


def mm_nt(a, b):
    return lax.dot_general(a, b, (((1,), (1,)), ((), ())), preferred_element_type=F32)


def cut_kernel(x_hbm, o_hbm, x_ref, o_ref, done):
    half = ROWS // 2
    rows = [pl.ds(i * half, half) for i in range(2)]
    into = [pltpu.make_async_copy(x_hbm.at[r], x_ref.at[r], done.at[0, i]) for i, r in enumerate(rows)]
    back = [pltpu.make_async_copy(o_ref.at[:, r], o_hbm.at[:, r], done.at[1, i]) for i, r in enumerate(rows)]
    for move in into:
        move.start()
    for i in range(2):
        into[i].wait()
        for e in range(EP):
            o_ref[e, i * half : (i + 1) * half] = x_ref[i * half : (i + 1) * half, e * COLS : (e + 1) * COLS]
        back[i].start()
    for move in back:
        move.wait()


def cut(tokens):
    return pl.pallas_call(
        cut_kernel,
        out_shape=jax.ShapeDtypeStruct((EP, ROWS, COLS), BF),
        in_specs=[HBM],
        out_specs=HBM,
        scratch_shapes=[
            pltpu.VMEM((ROWS, WIDTH), BF), pltpu.VMEM((EP, ROWS, COLS), BF), pltpu.SemaphoreType.DMA((2, 2)),
        ],
        compiler_params=grant(2),
    )(in_hbm(tokens))


def prepare_kernel(
    me_ref, *refs,
):
    sources, outs, scratch = refs[:10], refs[10:17], refs[17:27]
    done = refs[27]
    moves = [pltpu.make_async_copy(a, b, done.at[i]) for i, (a, b) in enumerate(zip(sources, scratch))]
    for move in moves:
        move.start()
    x_ref, gain_ref, in_ref, forget_ref, bias_ref, max_ref, norm_ref, route_ref, weight_ref, state_ref = scratch
    scale_ref, write_ref, new_max_ref, extra_ref, table_ref, old_norm_ref, old_ref = outs
    for move in moves[:-1]:
        move.wait()
    wide = x_ref[...].astype(F32)
    scale = lax.rsqrt(jnp.sum(wide * wide, axis=1, keepdims=True) / WIDTH + EPS)
    scale_ref[...] = jnp.broadcast_to(scale, (ROWS, HEAD))
    normed = (wide * scale * gain_ref[...]).astype(BF)
    head = lax.broadcasted_iota(I32, (ROWS, TP), 1) == me_ref[1]
    pick = lambda x: jnp.sum(jnp.where(head, x, 0.0), axis=1, keepdims=True)
    row = lax.broadcasted_iota(I32, (ROWS, ROWS), 0)
    lane = lax.broadcasted_iota(I32, (ROWS, ROWS), 1)
    upright = lambda x: jnp.sum(jnp.where(lane == row, x, jnp.zeros_like(x)), axis=1, keepdims=True)
    flat = lambda x: jnp.sum(jnp.where(lane == row, x, jnp.zeros_like(x)), axis=0, keepdims=True)
    gate_in = pick(mm_nt(normed, in_ref[...]))
    gate_forget = pick(mm_nt(normed, forget_ref[...]) + bias_ref[...])
    old_max = upright(max_ref[...])
    log_keep = jnp.minimum(gate_forget, 0.0) - jnp.log1p(jnp.exp(-jnp.abs(gate_forget)))
    new_max = jnp.maximum(log_keep + old_max, gate_in)
    new_max_ref[...] = flat(new_max)
    keep = jnp.broadcast_to(jnp.exp(log_keep + old_max - new_max), (ROWS, HEAD))
    write_ref[...] = jnp.broadcast_to(jnp.exp(gate_in - new_max), (ROWS, HEAD))
    old_norm_ref[...] = keep * norm_ref[...].reshape(ROWS, HEAD)

    place = lax.broadcasted_iota(I32, (ROWS, 128), 1) == (me_ref[0] % 4) * ROWS + lax.broadcasted_iota(
        I32, (ROWS, 128), 0
    )
    across = [route_ref[k : k + 1, :] for k in range(2)]
    column = [upright(x) for x in across]
    lines = []
    for k in range(2):
        same = (across[0] == column[k]).astype(I32) + (across[1] == column[k]).astype(I32)
        slot = jnp.sum(jnp.where(lane < row, same, 0), axis=1, keepdims=True)
        code = column[k] * 8 + slot
        table_ref[k : k + 1, :] = flat(code).astype(F32)
        lines.append(jnp.sum(jnp.where(place, code, 0), axis=0, keepdims=True))
    lines.append(jnp.zeros((6, 128), I32))
    extra_ref[...] = jnp.concatenate(lines, axis=0).astype(F32).astype(BF)
    weight = weight_ref[...]
    table_ref[2:4, :] = weight / jnp.sum(weight, axis=0, keepdims=True)
    moves[-1].wait()
    for r in range(ROWS):
        old_ref[r] = keep[r : r + 1] * state_ref[r, 0]


def prepare(me, *sources):
    wide = jax.ShapeDtypeStruct((ROWS, HEAD), F32)
    return pl.pallas_call(
        prepare_kernel,
        out_shape=(
            wide, wide, jax.ShapeDtypeStruct((1, ROWS), F32), jax.ShapeDtypeStruct((8, HEAD), BF),
            jax.ShapeDtypeStruct((4, ROWS), F32), wide, jax.ShapeDtypeStruct((ROWS, HEAD, HEAD), F32),
        ),
        in_specs=[SMEM] + [HBM] * 10,
        out_specs=(VMEM,) * 7,
        scratch_shapes=[pltpu.VMEM(x.shape, x.dtype) for x in sources] + [pltpu.SemaphoreType.DMA((10,))],
        compiler_params=grant(12),
    )(me, *[in_hbm(x) for x in sources])


def my_columns(ref, me_ref):
    return ref[:, pl.ds(pl.multiple_of(me_ref[0] * COLS, COLS), COLS)]


def heads_kernel(me_ref, x_ref, gain_ref, q_ref, k_ref, v_ref, g_ref, o_ref, mine_ref):
    x = (x_ref[...].reshape(ALL, COLS).astype(F32) * my_columns(gain_ref, me_ref)).astype(BF)
    for i, w in enumerate((q_ref, k_ref, v_ref, g_ref)):
        o_ref[:, :, i * HEAD : (i + 1) * HEAD] = mm(x, w[...]).astype(BF).reshape(EP, ROWS, HEAD)
    mine_ref[...] = x_ref[me_ref[1]]


def heads(me, token_cols, gain, ws):
    return pl.pallas_call(
        heads_kernel,
        out_shape=(
            jax.ShapeDtypeStruct((EP, ROWS, 4 * HEAD), BF),
            jax.ShapeDtypeStruct((ROWS, COLS), BF),
        ),
        in_specs=[SMEM] + [VMEM] * 6,
        out_specs=(VMEM, VMEM),
        compiler_params=grant(6),
    )(me, token_cols, gain, *ws)


STEP = 8


def cell_kernel(p_ref, scale_ref, write_ref, extra_ref, norm_ref, old_ref, mixed_ref, new_norm_ref, new_ref, numer):
    proj = []
    for i in range(4):
        lanes = slice(i * HEAD, (i + 1) * HEAD)
        total = p_ref[0, :, lanes].astype(F32)
        for e in range(1, EP):
            total = total + p_ref[e, :, lanes].astype(F32)
        proj.append(total * scale_ref[...])
    query, key, value, outgate = proj
    wkey = write_ref[...] * (key * HEAD ** (-0.5))
    new_norm = norm_ref[...] + wkey
    new_norm_ref[...] = new_norm
    for step in range(ROWS // STEP):
        here = slice(step * STEP, (step + 1) * STEP)
        query_t, wkey_t = query[here].T, wkey[here].T
        for j in range(STEP):
            row = step * STEP + j
            new = old_ref[row] + wkey_t[:, j : j + 1] * value[row : row + 1]
            new_ref[row, 0] = new
            numer[row : row + 1, :] = jnp.sum(query_t[:, j : j + 1] * new, axis=0, keepdims=True)
    denom = jnp.sum(query * new_norm, axis=1, keepdims=True)
    out = numer[...] / jnp.maximum(jnp.abs(denom), 1.0)
    mixed = (jax.nn.sigmoid(outgate) * out).astype(BF)
    extra = extra_ref[...]
    for e in range(EP):
        mixed_ref[e, :ROWS] = mixed
        mixed_ref[e, ROWS:] = extra


def cell(parts, scale, write, extra, norm, old):
    return pl.pallas_call(
        cell_kernel,
        out_shape=(
            jax.ShapeDtypeStruct((EP, ROWS + 8, HEAD), BF),
            pltpu.VMEM((ROWS, HEAD), F32),
            pltpu.VMEM((ROWS, 1, HEAD, HEAD), F32),
        ),
        in_specs=[VMEM] * 6,
        out_specs=(VMEM,) * 3,
        scratch_shapes=[pltpu.VMEM((ROWS, HEAD), F32)],
        compiler_params=grant(8),
    )(parts, scale, write, extra, norm, old)


def proj_kernel(me_ref, x_ref, w_ref, mine_ref, sent_ref, out):
    core = me_ref[1] % 2
    out[...] = mm(x_ref[:, :ROWS, :].reshape(ALL, HEAD), w_ref[...])
    for z in range(CHIPS):
        mine_ref[z] = out[pl.ds(pl.multiple_of((2 * z + core) * ROWS, ROWS), ROWS), :].astype(BF)
        sent_ref[z] = out[pl.ds(pl.multiple_of((2 * z + 1 - core) * ROWS, ROWS), ROWS), :].astype(BF)


def proj(me, mixed, w):
    part = jax.ShapeDtypeStruct((CHIPS, ROWS, COLS), BF)
    return pl.pallas_call(
        proj_kernel,
        out_shape=(part, part),
        in_specs=[SMEM, VMEM, VMEM],
        out_specs=(VMEM, VMEM),
        scratch_shapes=[pltpu.VMEM((ALL, COLS), F32)],
        compiler_params=grant(4),
    )(me, mixed, w)


def join_kernel(x_ref, y_ref, o_ref):
    o_ref[...] = (x_ref[...].astype(F32) + y_ref[...].astype(F32)).astype(BF)


def join(x, y):
    return pl.pallas_call(
        join_kernel,
        out_shape=jax.ShapeDtypeStruct(x.shape, BF),
        in_specs=[VMEM, VMEM],
        out_specs=VMEM,
        compiler_params=grant(2),
    )(x, y)


def settle_kernel(p_ref, base_ref, o_ref):
    total = p_ref[0].astype(F32)
    for z in range(1, CHIPS):
        total = total + p_ref[z].astype(F32)
    out = (base_ref[...].astype(F32) + total).astype(BF)
    for z in range(CHIPS):
        o_ref[z] = out


def settle(parts, base):
    return pl.pallas_call(
        settle_kernel,
        out_shape=jax.ShapeDtypeStruct(parts.shape, BF),
        in_specs=[VMEM, VMEM],
        out_specs=VMEM,
        compiler_params=grant(2),
    )(parts, base)


def high_low(x):
    high = x.astype(BF).astype(F32)
    return high, x - high


def feed_kernel(
    t_ref, r_ref, s_ref, gain_ref, branch_ref, mix_ref, gate_ref, up_ref, new_ref, norm_ref, o_ref, new_hbm, norm_hbm, whole, done,
):
    stores = [
        pltpu.make_async_copy(new_ref, new_hbm, done.at[0]), pltpu.make_async_copy(norm_ref, norm_hbm, done.at[1])
    ]
    for store in stores:
        store.start()
    core = t_ref[1] % 2
    for z in range(CHIPS):
        whole[2 * z + core] = r_ref[z]
        whole[2 * z + 1 - core] = s_ref[z]
    resid = whole[...].reshape(ALL, COLS)
    wide = resid.astype(F32)
    gained = (wide * my_columns(gain_ref, t_ref)).astype(BF)
    for half, w in enumerate((gate_ref, up_ref)):
        for j in range(4):
            part = mm(gained, w[:, j * 128 : (j + 1) * 128]).astype(BF).reshape(EP, ROWS, 128)
            at = ROUTED + (half * 4 + j) * ROWS
            o_ref[:, at : at + ROWS, :] = part
    square_high, square_low = high_low(wide * wide)
    ones = jnp.ones((8, COLS), BF)
    squares = mm_nt(ones, square_high.astype(BF)) + mm_nt(ones, square_low.astype(BF))
    line = lax.broadcasted_iota(I32, (2 * EP, 128), 0)
    pick = lambda h: jnp.sum(jnp.where(line == 2 * t_ref[0] + h, branch_ref[...].astype(F32), 0.0), axis=0, keepdims=True)
    weights = jnp.concatenate([pick(0), pick(1)], axis=1).astype(BF)
    branch = mm_nt(jnp.broadcast_to(weights, (8, COLS)), gained)
    sq_high, sq_low = high_low(squares)
    br_high, br_low = high_low(branch)
    line = lax.broadcasted_iota(I32, (8, ALL), 0)
    side = jnp.where(line == 0, sq_high, jnp.where(line == 1, sq_low, jnp.where(line == 2, br_high, br_low)))
    at = lax.broadcasted_iota(I32, (8 * EP, ALL), 0)
    token = lax.broadcasted_iota(I32, (8 * EP, ALL), 1)
    quarter = at % 8
    mine = (token == (at // 8) * ROWS + 2 * t_ref[1] + quarter // 2) & (quarter < 4)
    own = mm((mine & (quarter % 2 == 0)).astype(F32).astype(BF), resid[:, :128])
    own = own + mm((mine & (quarter % 2 == 1)).astype(F32).astype(BF), resid[:, 128:])
    for g in range(EP):
        tile = g // 4
        block = jnp.concatenate(
            [side[:, tile * 128 : (tile + 1) * 128], own[g * 8 : (g + 1) * 8]], axis=0
        )
        o_ref[g, SIDE:PACKED, :] = block.astype(BF)
    half_rows = CAP * EP // 2
    line = lax.broadcasted_iota(I32, (half_rows, 2 * 128), 0)
    base = (line // CAP) * 128 + line % CAP
    group = lax.broadcasted_iota(I32, (1, 2 * 128), 1) // ROWS
    for half in range(2):
        tiles = []
        for tile in (2 * half, 2 * half + 1):
            tiles.append(sum(mix_ref[4 * tile + i, ROWS:, :].astype(F32) for i in range(4)))
        codes = jnp.concatenate(tiles, axis=1).astype(I32)
        first = codes[0:1] + group * 128 - base
        second = codes[1:2] + group * 128 - base
        source = jnp.where(t_ref[1] % 2 == 0, wide[:, :128], wide[:, 128:])[half * 256 : (half + 1) * 256].astype(BF)
        for x in range(EP):
            member = (first == x * 8) | (second == x * 8)
            picked = mm(jnp.where(member, 1.0, 0.0).astype(BF), source).astype(BF)
            o_ref[x, half * half_rows : (half + 1) * half_rows, :] = picked
    for store in stores:
        store.wait()


def feed(me, resid, more, gain, branch, mix, gate, up, new_matrix, new_norm):
    return pl.pallas_call(
        feed_kernel,
        out_shape=(
            jax.ShapeDtypeStruct((EP, PACKED, 128), BF),
            jax.ShapeDtypeStruct(new_matrix.shape, F32),
            jax.ShapeDtypeStruct(new_norm.shape, F32),
        ),
        in_specs=[SMEM] + [VMEM] * 9,
        out_specs=(VMEM, HBM, HBM),
        scratch_shapes=[pltpu.VMEM((EP, ROWS, COLS), BF), pltpu.SemaphoreType.DMA((2,))],
        compiler_params=grant(14),
    )(me, resid, more, gain, branch, mix, gate, up, in_vmem(new_matrix), in_vmem(new_norm))


def over_peers(ref, at, size):
    value = ref[0, at : at + size, :].astype(F32)
    for e in range(1, EP):
        value = value + ref[e, at : at + size, :].astype(F32)
    return value


def token_sums(me_ref, side):
    lane = lax.broadcasted_iota(I32, (ROWS, 128), 1)
    row = lax.broadcasted_iota(I32, (ROWS, 128), 0)
    mine = lane == (me_ref[0] % 4) * ROWS + row
    squares = jnp.sum(jnp.where(mine, side[0:1] + side[1:2], 0.0), axis=1, keepdims=True)
    branch = jnp.sum(jnp.where(mine, side[2:3] + side[3:4], 0.0), axis=1, keepdims=True)
    return lax.rsqrt(squares / WIDTH + EPS), branch


def hidden_kernel(me_ref, p_ref, o_ref):
    scale, _ = token_sums(me_ref, over_peers(p_ref, SIDE, 16))
    for j in range(4):
        gate = over_peers(p_ref, ROUTED + j * ROWS, ROWS) * scale
        up = over_peers(p_ref, ROUTED + (4 + j) * ROWS, ROWS) * scale
        value = (gate * jax.nn.sigmoid(gate) * up).astype(BF)
        for e in range(EP):
            o_ref[e, :, j * 128 : (j + 1) * 128] = value


def hidden_units(me, packed):
    return pl.pallas_call(
        hidden_kernel,
        out_shape=jax.ShapeDtypeStruct((EP, ROWS, UNITS), BF),
        in_specs=[SMEM, VMEM],
        out_specs=VMEM,
        compiler_params=grant(8),
    )(me, packed)


def sides_kernel(me_ref, p_ref, b_ref, kept_ref, kept):
    scale, branch = token_sums(me_ref, over_peers(p_ref, SIDE, 16))
    b_ref[...] = jnp.broadcast_to(jax.nn.sigmoid(branch * scale), (ROWS, 128))
    for e in range(EP):
        rows = p_ref[e, SIDE:PACKED, :].astype(F32)
        for q in range(4):
            kept[q * EP + e : q * EP + e + 1, :] = rows[8 + q : 9 + q]
    kept_ref[...] = kept[...].astype(BF)


def sides(me, packed):
    return pl.pallas_call(
        sides_kernel,
        out_shape=(
            jax.ShapeDtypeStruct((ROWS, 128), F32),
            jax.ShapeDtypeStruct((2 * CHUNKS, 128), BF),
        ),
        in_specs=[SMEM, VMEM],
        out_specs=(VMEM, VMEM),
        scratch_shapes=[pltpu.VMEM((2 * CHUNKS, 128), F32)],
        compiler_params=grant(4),
    )(me, packed)


K_STEPS, N_STEPS = 8, 8
PER_STEP = EP // K_STEPS
DEEP = WIDTH // K_STEPS
LANES = WIDTH // N_STEPS


def expert_kernel(
    me_ref, x_ref, y_ref, gain_ref, gate_hbm, up_hbm, down_hbm, o_ref, send_ref, gate_ref, up_ref, down_ref, turned, done,
):
    slots = CAP * EP
    core = me_ref[1] % 2
    gates, ups, downs = [], [], []
    for i in range(K_STEPS):
        part = pl.ds(i * DEEP, DEEP)
        gates.append(pltpu.make_async_copy(gate_hbm.at[0, part, :], gate_ref.at[part, :], done.at[0, i]))
        ups.append(pltpu.make_async_copy(up_hbm.at[0, part, :], up_ref.at[part, :], done.at[1, i]))
    for i in range(N_STEPS):
        part = pl.ds(i * LANES, LANES)
        downs.append(pltpu.make_async_copy(down_hbm.at[0, :, part], down_ref.at[:, part], done.at[2, i]))
    for i in range(K_STEPS):
        gates[i].start()
        ups[i].start()
    for move in downs:
        move.start()
    squares = jnp.zeros((slots, 128), F32)
    gate = jnp.zeros((slots, COLS), F32)
    up = jnp.zeros((slots, COLS), F32)
    for i in range(K_STEPS):
        pieces = []
        for e in range(i * PER_STEP, (i + 1) * PER_STEP):
            for h in range(2):
                x = jnp.where(core == h, x_ref[e, :ROUTED, :].astype(F32), y_ref[e].astype(F32))
                squares += x * x
                at = (2 * e + h) * 128
                pieces.append((x * gain_ref[:, at : at + 128]).astype(BF))
        x = jnp.concatenate(pieces, axis=1)
        gates[i].wait()
        ups[i].wait()
        gate += mm(x, gate_ref[i * DEEP : (i + 1) * DEEP, :])
        up += mm(x, up_ref[i * DEEP : (i + 1) * DEEP, :])
    scale = lax.rsqrt(jnp.sum(squares, axis=1, keepdims=True) / WIDTH + EPS)
    gate = gate * scale
    hidden = (gate * jax.nn.sigmoid(gate) * (up * scale)).astype(BF)
    for i in range(N_STEPS):
        downs[i].wait()
        out = mm(hidden, down_ref[:, i * LANES : (i + 1) * LANES])
        for c in range(LANES // 128):
            chunk = i * (LANES // 128) + c
            at = (chunk % 2) * slots * EP + chunk // 2
            turned[pl.ds(at, slots, stride=EP), :] = out[:, c * 128 : (c + 1) * 128]
    for g in range(EP):
        mine = pl.multiple_of(core * slots * EP + g * BACK, BACK)
        other = pl.multiple_of((1 - core) * slots * EP + g * BACK, BACK)
        o_ref[g] = turned[pl.ds(mine, BACK), :].astype(BF)
        send_ref[g] = turned[pl.ds(other, BACK), :].astype(BF)


def expert(me, packed, other, gain, gate, up, down_w):
    rows = jax.ShapeDtypeStruct((EP, BACK, 128), BF)
    return pl.pallas_call(
        expert_kernel,
        out_shape=(rows, rows),
        in_specs=[SMEM, VMEM, VMEM, VMEM, HBM, HBM, HBM],
        out_specs=(VMEM, VMEM),
        scratch_shapes=[
            pltpu.VMEM((WIDTH, COLS), BF),
            pltpu.VMEM((WIDTH, COLS), BF),
            pltpu.VMEM((COLS, WIDTH), BF),
            pltpu.VMEM((CAP * EP * CHUNKS, 128), F32),
            pltpu.SemaphoreType.DMA((3, 8)),
        ],
        compiler_params=grant(16),
    )(me, packed, other, gain, in_hbm(gate), in_hbm(up), in_hbm(down_w))


def down_kernel(h_ref, w_ref, x_ref, y_ref, o_ref):
    for g in range(EP):
        o_ref[g, :BACK, :] = (x_ref[g].astype(F32) + y_ref[g].astype(F32)).astype(BF)
    out = mm(h_ref[...].reshape(ALL, UNITS), w_ref[...]).astype(BF)
    for h in range(2):
        at = BACK + h * ROWS
        o_ref[:, at : at + ROWS, :] = out[:, h * 128 : (h + 1) * 128].reshape(EP, ROWS, 128)


def down(hidden, w, rows, more):
    return pl.pallas_call(
        down_kernel,
        out_shape=jax.ShapeDtypeStruct((EP, RETURN, 128), BF),
        in_specs=[VMEM] * 4,
        out_specs=VMEM,
        compiler_params=grant(6),
    )(hidden, w, rows, more)


def gather_kernel(me_ref, table_ref, branch_ref, r_ref, mine_ref, sent_ref, dense, out):
    for h in range(2):
        for e in range(EP):
            at = (h * EP + e) * ROWS
            dense[at : at + ROWS, :] = r_ref[e, BACK + h * ROWS : BACK + (h + 1) * ROWS, :].astype(F32)
    mine = lax.broadcasted_iota(I32, (CHUNKS, 128), 0) // EP == me_ref[1] % 2
    for r in range(ROWS):
        total = jnp.zeros((EP, 128), F32)
        for k in range(2):
            code = table_ref[k, r].astype(I32)
            at = pl.multiple_of((code % 8) * EP, EP)
            total = total + table_ref[2 + k, r] * r_ref[code // 8, pl.ds(at, EP), :].astype(F32)
        total = jnp.where(mine, jnp.concatenate([total, total], axis=0), 0.0)
        total = total + branch_ref[r : r + 1, :] * dense[pl.ds(r, CHUNKS, stride=ROWS), :]
        out[r // 2, (r % 2) * CHUNKS : (r % 2 + 1) * CHUNKS, :] = total
    core = me_ref[1] % 2
    for z in range(CHIPS):
        mine_ref[z] = out[2 * z + core].astype(BF)
        sent_ref[z] = out[2 * z + 1 - core].astype(BF)


def gather(me, table, branch, returned):
    part = jax.ShapeDtypeStruct((CHIPS, 2 * CHUNKS, 128), BF)
    return pl.pallas_call(
        gather_kernel,
        out_shape=(part, part),
        in_specs=[SMEM, SMEM, VMEM, VMEM],
        out_specs=(VMEM, VMEM),
        scratch_shapes=[pltpu.VMEM((CHUNKS * ROWS, 128), F32), pltpu.VMEM((TP, 2 * CHUNKS, 128), F32)],
        compiler_params=grant(6),
    )(me, table, branch, returned)


def finish_kernel(p_ref, kept_ref, o_ref, turned):
    total = p_ref[0].astype(F32)
    for t in range(1, CHIPS):
        total = total + p_ref[t].astype(F32)
    total = total + kept_ref[...].astype(F32)
    for r in range(2):
        for h in range(2):
            at = r * CHUNKS + h * EP
            turned[pl.ds(r * CHUNKS + h, EP, stride=2), :] = total[at : at + EP]
    out = turned[...].astype(BF)
    for t in range(CHIPS):
        o_ref[t] = out


def finish(parts, kept):
    return pl.pallas_call(
        finish_kernel,
        out_shape=jax.ShapeDtypeStruct(parts.shape, BF),
        in_specs=[VMEM, VMEM],
        out_specs=VMEM,
        scratch_shapes=[pltpu.VMEM((2 * CHUNKS, 128), F32)],
        compiler_params=grant(4),
    )(parts, kept)


def place_kernel(me_ref, x_ref, y_ref, o_ref, rows):
    core = me_ref[1] % 2
    size = 2 * CHUNKS
    for z in range(CHIPS):
        rows[pl.ds(pl.multiple_of((2 * z + core) * size, size), size), :] = x_ref[z].astype(F32)
        rows[pl.ds(pl.multiple_of((2 * z + 1 - core) * size, size), size), :] = y_ref[z].astype(F32)
    for c in range(CHUNKS):
        o_ref[:, c * 128 : (c + 1) * 128] = rows[pl.ds(c, ROWS, stride=CHUNKS), :].astype(BF)


def place(me, mine, other):
    return pl.pallas_call(
        place_kernel,
        out_shape=jax.ShapeDtypeStruct((ROWS, WIDTH), BF),
        in_specs=[SMEM, VMEM, VMEM],
        out_specs=VMEM,
        scratch_shapes=[pltpu.VMEM((ROWS * CHUNKS, 128), F32)],
        compiler_params=grant(4),
    )(me, mine, other)


def on_device(
    tokens,
    state_matrix,
    state_norm,
    state_max,
    mixer_gain,
    w_query,
    w_key,
    w_value,
    w_outgate,
    w_ingate,
    w_forget,
    forget_bias,
    w_proj,
    ffn_gain,
    w_branch,
    routes,
    route_weight,
    expert_gate,
    expert_up,
    expert_down,
    dense_gate,
    dense_up,
    dense_down,
):
    me = jnp.stack([lax.axis_index("ep"), lax.axis_index("tp")]).astype(I32)
    token_cols = swap(cut(tokens), "ep")
    own = prepare(
        me, tokens, mixer_gain[None], w_ingate.T, w_forget.T, forget_bias[None], state_max.T, state_norm,
        routes.T, route_weight.T, state_matrix,
    )
    gains = (mixer_gain[None], ffn_gain[None], w_branch.reshape(2 * EP, 128))
    scale, write, new_max, extra, table, norm, old = own
    (token_cols, scale, write, extra, norm, old, gains, me) = lax.optimization_barrier(
        (token_cols, scale, write, extra, norm, old, gains, me)
    )
    partial, token_block = heads(me, token_cols, gains[0], (w_query, w_key, w_value, w_outgate))
    parts = swap(partial, "ep")
    mixed, new_norm, new_matrix = cell(parts, scale, write, extra, norm, old)
    mixed_all = swap(mixed, "ep")

    mine, sent = proj(me, mixed_all, w_proj)
    parts = swap_z(join(mine, from_core(sent)))
    resid = swap_z(settle(parts, token_block))
    more = from_core(resid)

    packed, new_matrix, new_norm = feed(
        me, resid, more, gains[1], gains[2], mixed_all, dense_gate, dense_up, new_matrix, new_norm
    )
    packed = swap(packed, "ep")
    other = from_core(packed[:, :ROUTED])
    hidden = hidden_units(me, packed)
    hidden_all = swap(hidden, "ep")

    _, packed, other = lax.optimization_barrier((hidden, packed, other))
    branch, kept = sides(me, packed)
    rows_out, rows_sent = expert(me, packed, other, gains[1], expert_gate, expert_up, expert_down)
    more = from_core(rows_sent)
    hidden_all, rows_out, more, branch, kept, new_max, new_norm, table = lax.optimization_barrier(
        (hidden_all, rows_out, more, branch, kept, new_max, new_norm, table)
    )

    returned = swap(down(hidden_all, dense_down, rows_out, more), "ep")
    mine, sent = gather(me, table, branch, returned)
    parts = swap_z(join(mine, from_core(sent)))
    done = swap_z(finish(parts, kept))
    layer_out = place(me, done, from_core(done))
    new_max = new_max.T
    return (layer_out, new_matrix, new_norm[:, None], new_max)


def solution(mesh):
    in_specs = (
        P("ep", None),
        P("ep", "tp", None, None),
        P("ep", "tp", None),
        P("ep", "tp"),
        P(),
        P("ep", "tp"),
        P("ep", "tp"),
        P("ep", "tp"),
        P("ep", "tp"),
        P(),
        P(),
        P(),
        P("tp", "ep"),
        P(),
        P(),
        P("ep", None),
        P("ep", None),
        P("ep", None, "tp"),
        P("ep", None, "tp"),
        P("ep", "tp", None),
        P("ep", "tp"),
        P("ep", "tp"),
        P("tp", "ep"),
    )
    out_specs = (P("ep", None), P("ep", "tp", None, None), P("ep", "tp", None), P("ep", "tp"))
    return jax.shard_map(
        on_device, mesh=mesh, in_specs=in_specs, out_specs=out_specs, check_vma=False
    )
```

```python
import jax
import jax.numpy as jnp
from jax import lax
from jax.experimental import pallas as pl
from jax.experimental.pallas import tpu as pltpu
from jax.sharding import PartitionSpec as P

EPS = 1e-06
BF = jnp.bfloat16
F32 = jnp.float32
I32 = jnp.int32
EP, TP = 16, 16
ROWS, WIDTH, COLS, HEAD, UNITS, CAP = 32, 4096, 256, 128, 512, 6
ALL = ROWS * EP
ROUTED = CAP * EP // 2
SIDE = ROUTED + 8 * ROWS
PACKED = SIDE + 16
CHUNKS = WIDTH // 128
BACK = CAP * EP
RETURN = BACK + 2 * ROWS


def in_hbm(x):
    return pltpu.with_memory_space_constraint(x, pltpu.HBM)


def in_vmem(x):
    return pltpu.with_memory_space_constraint(x, pltpu.VMEM)


def grant(mib):
    return pltpu.CompilerParams(vmem_limit_bytes=mib * 1024 * 1024)


VMEM = pl.BlockSpec(memory_space=pltpu.VMEM)
SMEM = pl.BlockSpec(memory_space=pltpu.SMEM)
HBM = pl.BlockSpec(memory_space=pltpu.HBM)


def swap(parts, axis):
    return lax.all_to_all(parts, axis, 0, 0, tiled=True)


CHIPS = TP // 2
ALONG_Z = [[2 * z + core for z in range(CHIPS)] for core in range(2)]
CORES = [(t, t ^ 1) for t in range(TP)]


def swap_z(parts):
    return lax.all_to_all(parts, "tp", 0, 0, tiled=True, axis_index_groups=ALONG_Z)


def from_core(x):
    return lax.ppermute(x, "tp", CORES)


def mm(a, b):
    return jnp.dot(a, b, preferred_element_type=F32)


def mm_nt(a, b):
    return lax.dot_general(a, b, (((1,), (1,)), ((), ())), preferred_element_type=F32)


def cut_kernel(x_hbm, o_hbm, x_ref, o_ref, done):
    half = ROWS // 2
    rows = [pl.ds(i * half, half) for i in range(2)]
    into = [pltpu.make_async_copy(x_hbm.at[r], x_ref.at[r], done.at[0, i]) for i, r in enumerate(rows)]
    back = [pltpu.make_async_copy(o_ref.at[:, r], o_hbm.at[:, r], done.at[1, i]) for i, r in enumerate(rows)]
    for move in into:
        move.start()
    for i in range(2):
        into[i].wait()
        for e in range(EP):
            o_ref[e, i * half : (i + 1) * half] = x_ref[i * half : (i + 1) * half, e * COLS : (e + 1) * COLS]
        back[i].start()
    for move in back:
        move.wait()


def cut(tokens):
    return pl.pallas_call(
        cut_kernel,
        out_shape=jax.ShapeDtypeStruct((EP, ROWS, COLS), BF),
        in_specs=[HBM],
        out_specs=HBM,
        scratch_shapes=[
            pltpu.VMEM((ROWS, WIDTH), BF), pltpu.VMEM((EP, ROWS, COLS), BF), pltpu.SemaphoreType.DMA((2, 2)),
        ],
        compiler_params=grant(2),
    )(in_hbm(tokens))


def prepare_kernel(
    me_ref, *refs,
):
    sources, outs, scratch = refs[:10], refs[10:17], refs[17:27]
    done = refs[27]
    moves = [pltpu.make_async_copy(a, b, done.at[i]) for i, (a, b) in enumerate(zip(sources, scratch))]
    for move in moves:
        move.start()
    x_ref, gain_ref, in_ref, forget_ref, bias_ref, max_ref, norm_ref, route_ref, weight_ref, state_ref = scratch
    scale_ref, write_ref, new_max_ref, extra_ref, table_ref, old_norm_ref, old_ref = outs
    for move in moves[:-1]:
        move.wait()
    wide = x_ref[...].astype(F32)
    scale = lax.rsqrt(jnp.sum(wide * wide, axis=1, keepdims=True) / WIDTH + EPS)
    scale_ref[...] = jnp.broadcast_to(scale, (ROWS, HEAD))
    normed = (wide * scale * gain_ref[...]).astype(BF)
    head = lax.broadcasted_iota(I32, (ROWS, TP), 1) == me_ref[1]
    pick = lambda x: jnp.sum(jnp.where(head, x, 0.0), axis=1, keepdims=True)
    row = lax.broadcasted_iota(I32, (ROWS, ROWS), 0)
    lane = lax.broadcasted_iota(I32, (ROWS, ROWS), 1)
    upright = lambda x: jnp.sum(jnp.where(lane == row, x, jnp.zeros_like(x)), axis=1, keepdims=True)
    flat = lambda x: jnp.sum(jnp.where(lane == row, x, jnp.zeros_like(x)), axis=0, keepdims=True)
    gate_in = pick(mm_nt(normed, in_ref[...]))
    gate_forget = pick(mm_nt(normed, forget_ref[...]) + bias_ref[...])
    old_max = upright(max_ref[...])
    log_keep = jnp.minimum(gate_forget, 0.0) - jnp.log1p(jnp.exp(-jnp.abs(gate_forget)))
    new_max = jnp.maximum(log_keep + old_max, gate_in)
    new_max_ref[...] = flat(new_max)
    keep = jnp.broadcast_to(jnp.exp(log_keep + old_max - new_max), (ROWS, HEAD))
    write_ref[...] = jnp.broadcast_to(jnp.exp(gate_in - new_max), (ROWS, HEAD))
    old_norm_ref[...] = keep * norm_ref[...].reshape(ROWS, HEAD)

    place = lax.broadcasted_iota(I32, (ROWS, 128), 1) == (me_ref[0] % 4) * ROWS + lax.broadcasted_iota(
        I32, (ROWS, 128), 0
    )
    across = [route_ref[k : k + 1, :] for k in range(2)]
    column = [upright(x) for x in across]
    lines = []
    for k in range(2):
        same = (across[0] == column[k]).astype(I32) + (across[1] == column[k]).astype(I32)
        slot = jnp.sum(jnp.where(lane < row, same, 0), axis=1, keepdims=True)
        code = column[k] * 8 + slot
        table_ref[k : k + 1, :] = flat(code).astype(F32)
        lines.append(jnp.sum(jnp.where(place, code, 0), axis=0, keepdims=True))
    lines.append(jnp.zeros((6, 128), I32))
    extra_ref[...] = jnp.concatenate(lines, axis=0).astype(F32).astype(BF)
    weight = weight_ref[...]
    table_ref[2:4, :] = weight / jnp.sum(weight, axis=0, keepdims=True)
    moves[-1].wait()
    for r in range(ROWS):
        old_ref[r] = keep[r : r + 1] * state_ref[r, 0]


def prepare(me, *sources):
    wide = jax.ShapeDtypeStruct((ROWS, HEAD), F32)
    return pl.pallas_call(
        prepare_kernel,
        out_shape=(
            wide, wide, jax.ShapeDtypeStruct((1, ROWS), F32), jax.ShapeDtypeStruct((8, HEAD), BF),
            jax.ShapeDtypeStruct((4, ROWS), F32), wide, jax.ShapeDtypeStruct((ROWS, HEAD, HEAD), F32),
        ),
        in_specs=[SMEM] + [HBM] * 10,
        out_specs=(VMEM,) * 7,
        scratch_shapes=[pltpu.VMEM(x.shape, x.dtype) for x in sources] + [pltpu.SemaphoreType.DMA((10,))],
        compiler_params=grant(12),
    )(me, *[in_hbm(x) for x in sources])


def my_columns(ref, me_ref):
    return ref[:, pl.ds(pl.multiple_of(me_ref[0] * COLS, COLS), COLS)]


def heads_kernel(me_ref, x_ref, gain_ref, q_ref, k_ref, v_ref, g_ref, o_ref, mine_ref):
    x = (x_ref[...].reshape(ALL, COLS).astype(F32) * my_columns(gain_ref, me_ref)).astype(BF)
    for i, w in enumerate((q_ref, k_ref, v_ref, g_ref)):
        o_ref[:, :, i * HEAD : (i + 1) * HEAD] = mm(x, w[...]).astype(BF).reshape(EP, ROWS, HEAD)
    mine_ref[...] = x_ref[me_ref[1]]


def heads(me, token_cols, gain, ws):
    return pl.pallas_call(
        heads_kernel,
        out_shape=(
            jax.ShapeDtypeStruct((EP, ROWS, 4 * HEAD), BF),
            jax.ShapeDtypeStruct((ROWS, COLS), BF),
        ),
        in_specs=[SMEM] + [VMEM] * 6,
        out_specs=(VMEM, VMEM),
        compiler_params=grant(6),
    )(me, token_cols, gain, *ws)


STEP = 8


def cell_kernel(p_ref, scale_ref, write_ref, extra_ref, norm_ref, old_ref, mixed_ref, new_norm_ref, new_ref, numer):
    proj = []
    for i in range(4):
        lanes = slice(i * HEAD, (i + 1) * HEAD)
        total = p_ref[0, :, lanes].astype(F32)
        for e in range(1, EP):
            total = total + p_ref[e, :, lanes].astype(F32)
        proj.append(total * scale_ref[...])
    query, key, value, outgate = proj
    wkey = write_ref[...] * (key * HEAD ** (-0.5))
    new_norm = norm_ref[...] + wkey
    new_norm_ref[...] = new_norm
    for step in range(ROWS // STEP):
        here = slice(step * STEP, (step + 1) * STEP)
        query_t, wkey_t = query[here].T, wkey[here].T
        for j in range(STEP):
            row = step * STEP + j
            new = old_ref[row] + wkey_t[:, j : j + 1] * value[row : row + 1]
            new_ref[row, 0] = new
            numer[row : row + 1, :] = jnp.sum(query_t[:, j : j + 1] * new, axis=0, keepdims=True)
    denom = jnp.sum(query * new_norm, axis=1, keepdims=True)
    out = numer[...] / jnp.maximum(jnp.abs(denom), 1.0)
    mixed = (jax.nn.sigmoid(outgate) * out).astype(BF)
    extra = extra_ref[...]
    for e in range(EP):
        mixed_ref[e, :ROWS] = mixed
        mixed_ref[e, ROWS:] = extra


def cell(parts, scale, write, extra, norm, old):
    return pl.pallas_call(
        cell_kernel,
        out_shape=(
            jax.ShapeDtypeStruct((EP, ROWS + 8, HEAD), BF),
            pltpu.VMEM((ROWS, HEAD), F32),
            pltpu.VMEM((ROWS, 1, HEAD, HEAD), F32),
        ),
        in_specs=[VMEM] * 6,
        out_specs=(VMEM,) * 3,
        scratch_shapes=[pltpu.VMEM((ROWS, HEAD), F32)],
        compiler_params=grant(8),
    )(parts, scale, write, extra, norm, old)


def proj_kernel(me_ref, x_ref, w_ref, mine_ref, sent_ref, out):
    core = me_ref[1] % 2
    out[...] = mm(x_ref[:, :ROWS, :].reshape(ALL, HEAD), w_ref[...])
    for z in range(CHIPS):
        mine_ref[z] = out[pl.ds(pl.multiple_of((2 * z + core) * ROWS, ROWS), ROWS), :].astype(BF)
        sent_ref[z] = out[pl.ds(pl.multiple_of((2 * z + 1 - core) * ROWS, ROWS), ROWS), :].astype(BF)


def proj(me, mixed, w):
    part = jax.ShapeDtypeStruct((CHIPS, ROWS, COLS), BF)
    return pl.pallas_call(
        proj_kernel,
        out_shape=(part, part),
        in_specs=[SMEM, VMEM, VMEM],
        out_specs=(VMEM, VMEM),
        scratch_shapes=[pltpu.VMEM((ALL, COLS), F32)],
        compiler_params=grant(4),
    )(me, mixed, w)


def join_kernel(x_ref, y_ref, o_ref):
    o_ref[...] = (x_ref[...].astype(F32) + y_ref[...].astype(F32)).astype(BF)


def join(x, y):
    return pl.pallas_call(
        join_kernel,
        out_shape=jax.ShapeDtypeStruct(x.shape, BF),
        in_specs=[VMEM, VMEM],
        out_specs=VMEM,
        compiler_params=grant(2),
    )(x, y)


def settle_kernel(p_ref, base_ref, o_ref):
    total = p_ref[0].astype(F32)
    for z in range(1, CHIPS):
        total = total + p_ref[z].astype(F32)
    out = (base_ref[...].astype(F32) + total).astype(BF)
    for z in range(CHIPS):
        o_ref[z] = out


def settle(parts, base):
    return pl.pallas_call(
        settle_kernel,
        out_shape=jax.ShapeDtypeStruct(parts.shape, BF),
        in_specs=[VMEM, VMEM],
        out_specs=VMEM,
        compiler_params=grant(2),
    )(parts, base)


def high_low(x):
    high = x.astype(BF).astype(F32)
    return high, x - high


def feed_kernel(
    t_ref, r_ref, s_ref, gain_ref, branch_ref, mix_ref, gate_ref, up_ref, new_ref, norm_ref, o_ref, new_hbm, norm_hbm, whole, done,
):
    stores = [
        pltpu.make_async_copy(new_ref, new_hbm, done.at[0]), pltpu.make_async_copy(norm_ref, norm_hbm, done.at[1])
    ]
    for store in stores:
        store.start()
    core = t_ref[1] % 2
    for z in range(CHIPS):
        whole[2 * z + core] = r_ref[z]
        whole[2 * z + 1 - core] = s_ref[z]
    resid = whole[...].reshape(ALL, COLS)
    wide = resid.astype(F32)
    gained = (wide * my_columns(gain_ref, t_ref)).astype(BF)
    for half, w in enumerate((gate_ref, up_ref)):
        for j in range(4):
            part = mm(gained, w[:, j * 128 : (j + 1) * 128]).astype(BF).reshape(EP, ROWS, 128)
            at = ROUTED + (half * 4 + j) * ROWS
            o_ref[:, at : at + ROWS, :] = part
    square_high, square_low = high_low(wide * wide)
    ones = jnp.ones((8, COLS), BF)
    squares = mm_nt(ones, square_high.astype(BF)) + mm_nt(ones, square_low.astype(BF))
    line = lax.broadcasted_iota(I32, (2 * EP, 128), 0)
    pick = lambda h: jnp.sum(jnp.where(line == 2 * t_ref[0] + h, branch_ref[...].astype(F32), 0.0), axis=0, keepdims=True)
    weights = jnp.concatenate([pick(0), pick(1)], axis=1).astype(BF)
    branch = mm_nt(jnp.broadcast_to(weights, (8, COLS)), gained)
    sq_high, sq_low = high_low(squares)
    br_high, br_low = high_low(branch)
    line = lax.broadcasted_iota(I32, (8, ALL), 0)
    side = jnp.where(line == 0, sq_high, jnp.where(line == 1, sq_low, jnp.where(line == 2, br_high, br_low)))
    at = lax.broadcasted_iota(I32, (8 * EP, ALL), 0)
    token = lax.broadcasted_iota(I32, (8 * EP, ALL), 1)
    quarter = at % 8
    mine = (token == (at // 8) * ROWS + 2 * t_ref[1] + quarter // 2) & (quarter < 4)
    own = mm((mine & (quarter % 2 == 0)).astype(F32).astype(BF), resid[:, :128])
    own = own + mm((mine & (quarter % 2 == 1)).astype(F32).astype(BF), resid[:, 128:])
    for g in range(EP):
        tile = g // 4
        block = jnp.concatenate(
            [side[:, tile * 128 : (tile + 1) * 128], own[g * 8 : (g + 1) * 8]], axis=0
        )
        o_ref[g, SIDE:PACKED, :] = block.astype(BF)
    line = lax.broadcasted_iota(I32, (ROUTED, 2 * 128), 0)
    base = (line // CAP) * 128 + line % CAP
    group = lax.broadcasted_iota(I32, (1, 2 * 128), 1) // ROWS
    start = 8 * ((t_ref[1] // 2) % 2)
    tiles = []
    for tile in range(2):
        tiles.append(sum(mix_ref[start + 4 * tile + i, ROWS:, :].astype(F32) for i in range(4)))
    codes = jnp.concatenate(tiles, axis=1).astype(I32)
    first = codes[0:1] + group * 128 - base
    second = codes[1:2] + group * 128 - base
    source = jnp.where(core == 0, wide[:, :128], wide[:, 128:])
    source = jnp.where(start == 0, source[:256], source[256:]).astype(BF)
    for x in range(EP):
        member = (first == x * 8) | (second == x * 8)
        o_ref[x, :ROUTED, :] = mm(jnp.where(member, 1.0, 0.0).astype(BF), source).astype(BF)
    for store in stores:
        store.wait()


def feed(me, resid, more, gain, branch, mix, gate, up, new_matrix, new_norm):
    return pl.pallas_call(
        feed_kernel,
        out_shape=(
            jax.ShapeDtypeStruct((EP, PACKED, 128), BF),
            jax.ShapeDtypeStruct(new_matrix.shape, F32),
            jax.ShapeDtypeStruct(new_norm.shape, F32),
        ),
        in_specs=[SMEM] + [VMEM] * 9,
        out_specs=(VMEM, HBM, HBM),
        scratch_shapes=[pltpu.VMEM((EP, ROWS, COLS), BF), pltpu.SemaphoreType.DMA((2,))],
        compiler_params=grant(14),
    )(me, resid, more, gain, branch, mix, gate, up, in_vmem(new_matrix), in_vmem(new_norm))


def over_peers(ref, at, size):
    value = ref[0, at : at + size, :].astype(F32)
    for e in range(1, EP):
        value = value + ref[e, at : at + size, :].astype(F32)
    return value


def token_sums(me_ref, side):
    lane = lax.broadcasted_iota(I32, (ROWS, 128), 1)
    row = lax.broadcasted_iota(I32, (ROWS, 128), 0)
    mine = lane == (me_ref[0] % 4) * ROWS + row
    squares = jnp.sum(jnp.where(mine, side[0:1] + side[1:2], 0.0), axis=1, keepdims=True)
    branch = jnp.sum(jnp.where(mine, side[2:3] + side[3:4], 0.0), axis=1, keepdims=True)
    return lax.rsqrt(squares / WIDTH + EPS), branch


def hidden_kernel(me_ref, p_ref, o_ref):
    scale, _ = token_sums(me_ref, over_peers(p_ref, SIDE, 16))
    for j in range(4):
        gate = over_peers(p_ref, ROUTED + j * ROWS, ROWS) * scale
        up = over_peers(p_ref, ROUTED + (4 + j) * ROWS, ROWS) * scale
        value = (gate * jax.nn.sigmoid(gate) * up).astype(BF)
        for e in range(EP):
            o_ref[e, :, j * 128 : (j + 1) * 128] = value


def hidden_units(me, packed):
    return pl.pallas_call(
        hidden_kernel,
        out_shape=jax.ShapeDtypeStruct((EP, ROWS, UNITS), BF),
        in_specs=[SMEM, VMEM],
        out_specs=VMEM,
        compiler_params=grant(8),
    )(me, packed)


def sides_kernel(me_ref, p_ref, b_ref, kept_ref, kept):
    scale, branch = token_sums(me_ref, over_peers(p_ref, SIDE, 16))
    b_ref[...] = jnp.broadcast_to(jax.nn.sigmoid(branch * scale), (ROWS, 128))
    for e in range(EP):
        rows = p_ref[e, SIDE:PACKED, :].astype(F32)
        for q in range(4):
            kept[q * EP + e : q * EP + e + 1, :] = rows[8 + q : 9 + q]
    kept_ref[...] = kept[...].astype(BF)


def sides(me, packed):
    return pl.pallas_call(
        sides_kernel,
        out_shape=(
            jax.ShapeDtypeStruct((ROWS, 128), F32),
            jax.ShapeDtypeStruct((2 * CHUNKS, 128), BF),
        ),
        in_specs=[SMEM, VMEM],
        out_specs=(VMEM, VMEM),
        scratch_shapes=[pltpu.VMEM((2 * CHUNKS, 128), F32)],
        compiler_params=grant(4),
    )(me, packed)


K_STEPS, N_STEPS = 8, 8
PER_STEP = EP // K_STEPS
DEEP = WIDTH // K_STEPS
LANES = WIDTH // N_STEPS


def expert_kernel(
    me_ref, x_ref, y_ref, gain_ref, gate_hbm, up_hbm, down_hbm, o_ref, send_ref, gate_ref, up_ref, down_ref, turned, done,
):
    slots = CAP * EP
    core = me_ref[1] % 2
    gates, ups, downs = [], [], []
    for i in range(K_STEPS):
        part = pl.ds(i * DEEP, DEEP)
        gates.append(pltpu.make_async_copy(gate_hbm.at[0, part, :], gate_ref.at[part, :], done.at[0, i]))
        ups.append(pltpu.make_async_copy(up_hbm.at[0, part, :], up_ref.at[part, :], done.at[1, i]))
    for i in range(N_STEPS):
        part = pl.ds(i * LANES, LANES)
        downs.append(pltpu.make_async_copy(down_hbm.at[0, :, part], down_ref.at[:, part], done.at[2, i]))
    for i in range(K_STEPS):
        gates[i].start()
        ups[i].start()
    for move in downs:
        move.start()
    squares = jnp.zeros((slots, 128), F32)
    gate = jnp.zeros((slots, COLS), F32)
    up = jnp.zeros((slots, COLS), F32)
    for i in range(K_STEPS):
        pieces = []
        for e in range(i * PER_STEP, (i + 1) * PER_STEP):
            for h in range(2):
                x = jnp.where(core == h, x_ref[e].astype(F32), y_ref[e].astype(F32))
                squares += x * x
                at = (2 * e + h) * 128
                pieces.append((x * gain_ref[:, at : at + 128]).astype(BF))
        x = jnp.concatenate(pieces, axis=1)
        gates[i].wait()
        ups[i].wait()
        gate += mm(x, gate_ref[i * DEEP : (i + 1) * DEEP, :])
        up += mm(x, up_ref[i * DEEP : (i + 1) * DEEP, :])
    scale = lax.rsqrt(jnp.sum(squares, axis=1, keepdims=True) / WIDTH + EPS)
    gate = gate * scale
    hidden = (gate * jax.nn.sigmoid(gate) * (up * scale)).astype(BF)
    for i in range(N_STEPS):
        downs[i].wait()
        out = mm(hidden, down_ref[:, i * LANES : (i + 1) * LANES])
        for c in range(LANES // 128):
            chunk = i * (LANES // 128) + c
            at = (chunk % 2) * slots * EP + chunk // 2
            turned[pl.ds(at, slots, stride=EP), :] = out[:, c * 128 : (c + 1) * 128]
    start = 8 * ((me_ref[1] // 2) % 2)
    for g in range(EP):
        mine = pl.multiple_of(core * slots * EP + g * BACK, BACK)
        other = pl.multiple_of((1 - core) * slots * EP + g * BACK, BACK)
        to = start + g if g < 8 else g - start
        o_ref[to] = turned[pl.ds(mine, BACK), :].astype(BF)
        send_ref[to] = turned[pl.ds(other, BACK), :].astype(BF)


def expert(me, packed, other, gain, gate, up, down_w):
    rows = jax.ShapeDtypeStruct((EP, BACK, 128), BF)
    return pl.pallas_call(
        expert_kernel,
        out_shape=(rows, rows),
        in_specs=[SMEM, VMEM, VMEM, VMEM, HBM, HBM, HBM],
        out_specs=(VMEM, VMEM),
        scratch_shapes=[
            pltpu.VMEM((WIDTH, COLS), BF),
            pltpu.VMEM((WIDTH, COLS), BF),
            pltpu.VMEM((COLS, WIDTH), BF),
            pltpu.VMEM((CAP * EP * CHUNKS, 128), F32),
            pltpu.SemaphoreType.DMA((3, 8)),
        ],
        compiler_params=grant(16),
    )(me, packed, other, gain, in_hbm(gate), in_hbm(up), in_hbm(down_w))


def down_kernel(h_ref, w_ref, x_ref, y_ref, o_ref):
    for g in range(EP):
        o_ref[g, :BACK, :] = (x_ref[g].astype(F32) + y_ref[g].astype(F32)).astype(BF)
    out = mm(h_ref[...].reshape(ALL, UNITS), w_ref[...]).astype(BF)
    for h in range(2):
        at = BACK + h * ROWS
        o_ref[:, at : at + ROWS, :] = out[:, h * 128 : (h + 1) * 128].reshape(EP, ROWS, 128)


def down(hidden, w, rows, more):
    return pl.pallas_call(
        down_kernel,
        out_shape=jax.ShapeDtypeStruct((EP, RETURN, 128), BF),
        in_specs=[VMEM] * 4,
        out_specs=VMEM,
        compiler_params=grant(6),
    )(hidden, w, rows, more)


def gather_kernel(me_ref, table_ref, branch_ref, r_ref, mine_ref, sent_ref, dense, out):
    for h in range(2):
        for e in range(EP):
            at = (h * EP + e) * ROWS
            dense[at : at + ROWS, :] = r_ref[e, BACK + h * ROWS : BACK + (h + 1) * ROWS, :].astype(F32)
    mine = lax.broadcasted_iota(I32, (CHUNKS, 128), 0) // EP == me_ref[1] % 2
    for r in range(ROWS):
        total = jnp.zeros((EP, 128), F32)
        for k in range(2):
            code = table_ref[k, r].astype(I32)
            at = pl.multiple_of((code % 8) * EP, EP)
            total = total + table_ref[2 + k, r] * r_ref[code // 8, pl.ds(at, EP), :].astype(F32)
        total = jnp.where(mine, jnp.concatenate([total, total], axis=0), 0.0)
        total = total + branch_ref[r : r + 1, :] * dense[pl.ds(r, CHUNKS, stride=ROWS), :]
        out[r // 2, (r % 2) * CHUNKS : (r % 2 + 1) * CHUNKS, :] = total
    core = me_ref[1] % 2
    for z in range(CHIPS):
        mine_ref[z] = out[2 * z + core].astype(BF)
        sent_ref[z] = out[2 * z + 1 - core].astype(BF)


def gather(me, table, branch, returned):
    part = jax.ShapeDtypeStruct((CHIPS, 2 * CHUNKS, 128), BF)
    return pl.pallas_call(
        gather_kernel,
        out_shape=(part, part),
        in_specs=[SMEM, SMEM, VMEM, VMEM],
        out_specs=(VMEM, VMEM),
        scratch_shapes=[pltpu.VMEM((CHUNKS * ROWS, 128), F32), pltpu.VMEM((TP, 2 * CHUNKS, 128), F32)],
        compiler_params=grant(6),
    )(me, table, branch, returned)


def finish_kernel(p_ref, kept_ref, o_ref, turned):
    total = p_ref[0].astype(F32)
    for t in range(1, CHIPS):
        total = total + p_ref[t].astype(F32)
    total = total + kept_ref[...].astype(F32)
    for r in range(2):
        for h in range(2):
            at = r * CHUNKS + h * EP
            turned[pl.ds(r * CHUNKS + h, EP, stride=2), :] = total[at : at + EP]
    out = turned[...].astype(BF)
    for t in range(CHIPS):
        o_ref[t] = out


def finish(parts, kept):
    return pl.pallas_call(
        finish_kernel,
        out_shape=jax.ShapeDtypeStruct(parts.shape, BF),
        in_specs=[VMEM, VMEM],
        out_specs=VMEM,
        scratch_shapes=[pltpu.VMEM((2 * CHUNKS, 128), F32)],
        compiler_params=grant(4),
    )(parts, kept)


def place_kernel(me_ref, x_ref, y_ref, o_ref, rows):
    core = me_ref[1] % 2
    size = 2 * CHUNKS
    for z in range(CHIPS):
        rows[pl.ds(pl.multiple_of((2 * z + core) * size, size), size), :] = x_ref[z].astype(F32)
        rows[pl.ds(pl.multiple_of((2 * z + 1 - core) * size, size), size), :] = y_ref[z].astype(F32)
    for c in range(CHUNKS):
        o_ref[:, c * 128 : (c + 1) * 128] = rows[pl.ds(c, ROWS, stride=CHUNKS), :].astype(BF)


def place(me, mine, other):
    return pl.pallas_call(
        place_kernel,
        out_shape=jax.ShapeDtypeStruct((ROWS, WIDTH), BF),
        in_specs=[SMEM, VMEM, VMEM],
        out_specs=VMEM,
        scratch_shapes=[pltpu.VMEM((ROWS * CHUNKS, 128), F32)],
        compiler_params=grant(4),
    )(me, mine, other)


def on_device(
    tokens,
    state_matrix,
    state_norm,
    state_max,
    mixer_gain,
    w_query,
    w_key,
    w_value,
    w_outgate,
    w_ingate,
    w_forget,
    forget_bias,
    w_proj,
    ffn_gain,
    w_branch,
    routes,
    route_weight,
    expert_gate,
    expert_up,
    expert_down,
    dense_gate,
    dense_up,
    dense_down,
):
    me = jnp.stack([lax.axis_index("ep"), lax.axis_index("tp")]).astype(I32)
    token_cols = swap(cut(tokens), "ep")
    own = prepare(
        me, tokens, mixer_gain[None], w_ingate.T, w_forget.T, forget_bias[None], state_max.T, state_norm,
        routes.T, route_weight.T, state_matrix,
    )
    gains = (mixer_gain[None], ffn_gain[None], w_branch.reshape(2 * EP, 128))
    scale, write, new_max, extra, table, norm, old = own
    (token_cols, scale, write, extra, norm, old, gains, me) = lax.optimization_barrier(
        (token_cols, scale, write, extra, norm, old, gains, me)
    )
    partial, token_block = heads(me, token_cols, gains[0], (w_query, w_key, w_value, w_outgate))
    parts = swap(partial, "ep")
    mixed, new_norm, new_matrix = cell(parts, scale, write, extra, norm, old)
    mixed_all = swap(mixed, "ep")

    mine, sent = proj(me, mixed_all, w_proj)
    parts = swap_z(join(mine, from_core(sent)))
    resid = swap_z(settle(parts, token_block))
    more = from_core(resid)

    packed, new_matrix, new_norm = feed(
        me, resid, more, gains[1], gains[2], mixed_all, dense_gate, dense_up, new_matrix, new_norm
    )
    packed = swap(packed, "ep")
    quarter = packed[:, :ROUTED]
    beside = lax.ppermute(quarter, "tp", [(t, t ^ 2) for t in range(TP)])
    hidden = hidden_units(me, packed)
    hidden_all = swap(hidden, "ep")
    _, packed = lax.optimization_barrier((hidden, packed))
    branch, kept = sides(me, packed)
    pair = jnp.concatenate([quarter, beside], axis=1)
    other = from_core(pair)

    rows_out, rows_sent = expert(me, pair, other, gains[1], expert_gate, expert_up, expert_down)
    more = from_core(rows_sent)
    hidden_all, rows_out, more, branch, kept, new_max, new_norm, table = lax.optimization_barrier(
        (hidden_all, rows_out, more, branch, kept, new_max, new_norm, table)
    )

    returned = swap(down(hidden_all, dense_down, rows_out, more), "ep")
    mine, sent = gather(me, table, branch, returned)
    parts = swap_z(join(mine, from_core(sent)))
    done = swap_z(finish(parts, kept))
    layer_out = place(me, done, from_core(done))
    new_max = new_max.T
    return (layer_out, new_matrix, new_norm[:, None], new_max)


def solution(mesh):
    in_specs = (
        P("ep", None),
        P("ep", "tp", None, None),
        P("ep", "tp", None),
        P("ep", "tp"),
        P(),
        P("ep", "tp"),
        P("ep", "tp"),
        P("ep", "tp"),
        P("ep", "tp"),
        P(),
        P(),
        P(),
        P("tp", "ep"),
        P(),
        P(),
        P("ep", None),
        P("ep", None),
        P("ep", None, "tp"),
        P("ep", None, "tp"),
        P("ep", "tp", None),
        P("ep", "tp"),
        P("ep", "tp"),
        P("tp", "ep"),
    )
    out_specs = (P("ep", None), P("ep", "tp", None, None), P("ep", "tp", None), P("ep", "tp"))
    return jax.shard_map(
        on_device, mesh=mesh, in_specs=in_specs, out_specs=out_specs, check_vma=False
    )
```
